512 devices in a mesh: sp: 64 (over z, y), tp: 8 (over x, core).
Axes of the slice: x: 4, y: 4, z: 16, core: 2. Of those that a mesh axis runs over, the one named last changes fastest.
Arguments:
- queries: bfloat16 [8192, 768], P('sp', 'tp'), may hold values from -6 to 6
- latents: bfloat16 [8192, 512], P('sp'), may hold values from -6 to 6
- rot_key: bfloat16 [8192, 32], P('sp'), may hold values from -6 to 6
- kv_weight: bfloat16 [512, 1024], P(None, 'tp'), may hold values from -0.25 to 0.25
- log_sums: float32 [8192, 8], P('sp', 'tp'), may hold values from 4 to 14, as said below
- outputs: bfloat16 [8192, 512], P('sp', 'tp'), may hold values from -4 to 4
- out_grad: bfloat16 [8192, 512], P('sp', 'tp'), may hold values from -384 to 384
Outputs:
- query_grad: bfloat16 [8192, 768], P('sp', 'tp')
- key_grad: bfloat16 [8192, 512], P('sp', 'tp')
- value_grad: bfloat16 [8192, 512], P('sp', 'tp')
- rot_grad: float32 [8192, 32], P('sp')
- weight_grad: float32 [512, 1024], P('sp', 'tp')
The draws below stay inside these ranges and needn't reach their ends.
Inputs may be any that keep to these rules, and one draw needn't show every extreme that they name: `log_sums`: each value lies within one half of log(8192) + 0.5.
All inputs are finite; a program needn't handle non-finite values.
Results may differ from the reference program's by a relative error of at most 0.004.
The reference program's roundings to bfloat16 on the way (of `joined`, `key_full`, `probs_b` and `dscore`) count: a program that leaves them out, or rounds other values in their place, can miss the bound.
Values may be sent and summed in bfloat16 or wider, within the bound.
No kernel may reach another device: no remote copies, remote signals or barrier semaphores. Data moves between devices by JAX's collectives and lax.ppermute only.
A program may use at most 64 MiB of HBM per device.

```python
import math
import jax
import jax.numpy as jnp
from jax import lax

HEADS = 8
RANK = 512
NOPE_DIM = 64
ROPE_DIM = 32
VALUE_DIM = 64
SEQ = 8192


def draw_log_sums(key, part):
    center = math.log(SEQ) + 0.5
    return center + jax.random.uniform(key, (SEQ, HEADS), jnp.float32, -0.5, 0.5)


def with_spikes(result, own_key, source, target, parts, factor):
    def block_of(dim):
        return (jnp.arange(result.shape[dim]) // (result.shape[dim] // parts)).reshape((-1,) + (1,) * (result.ndim - 1 - dim))

    near = jax.random.permutation(own_key, parts)[block_of(target)]
    other_side = (block_of(target) + parts // 2) % parts
    return jnp.where((block_of(source) == near) | (block_of(source) == other_side), factor * result, result)


def block_scale(rng, dims, split, low, top_value):
    def one(dim, blocks):
        draws = jax.random.uniform(jax.random.fold_in(jax.random.fold_in(rng, 6), dim), (blocks,), jnp.float32, low / len(split), top_value / len(split))
        return jnp.repeat(jnp.exp(draws), dims[dim] // blocks).reshape((-1,) + (1,) * (len(dims) - dim - 1))

    loudness = one(*split[0])
    for cut in split[1:]:
        loudness = loudness * one(*cut)
    return loudness


def normal_values(key, shape, deviation, reach, shards=(), kind=jnp.bfloat16):
    array = jax.random.normal(key, shape, jnp.float32) * deviation
    if len(shards) > 0:
        array = block_scale(key, shape, shards, -0.22, 0.18) * array
    return jnp.clip(array, min=-reach, max=reach).astype(kind)


def noise_with(own_key, extent, spread, limit, pieces, heavy, held_as=jnp.bfloat16):
    entries = spread * jax.random.normal(own_key, extent, jnp.float32)
    if pieces:
        entries = entries * block_scale(own_key, extent, pieces, -0.22, 0.18)
    return jnp.clip(with_spikes(entries, jax.random.fold_in(own_key, 3), *heavy), -limit, limit).astype(held_as)


def setup_inputs(seed: int = 0) -> dict:
    splits = jax.random.split(jax.random.key(seed), 8)
    queries = normal_values(splits[0], (SEQ, HEADS * (NOPE_DIM + ROPE_DIM)), 1.0, 6.0, ((0, 64), (1, 8)))
    latents = normal_values(splits[1], (SEQ, RANK), 1.0, 6.0, ((0, 64),))
    rot_key = normal_values(splits[2], (SEQ, ROPE_DIM), 1.0, 6.0, ((0, 64),))
    kv_weight = normal_values(splits[3], (RANK, HEADS * (NOPE_DIM + VALUE_DIM)), RANK ** -0.5, 0.25, ((1, 8),))
    log_sums = draw_log_sums(jax.random.fold_in(splits[7], 71), 0)
    outputs = normal_values(splits[5], (SEQ, HEADS * VALUE_DIM), 0.3, 4.0, ((0, 64), (1, 8)))
    out_grad = noise_with(splits[6], (SEQ, HEADS * VALUE_DIM), (SEQ ** 0.5 / 4), 384.0, ((0, 64), (1, 8)), (0, 1, 64, 4.0))
    return dict(queries=queries, latents=latents, rot_key=rot_key, kv_weight=kv_weight, log_sums=log_sums, outputs=outputs, out_grad=out_grad)


def round_keep(values):
    rounded = values.astype(jnp.bfloat16)
    rounded = lax.optimization_barrier(rounded)
    return rounded.astype(jnp.float32)


def reference(queries, latents, rot_key, kv_weight, log_sums, outputs, out_grad):
    head_dim = NOPE_DIM + ROPE_DIM
    score_scale = head_dim ** -0.5
    joined = jnp.dot(latents, kv_weight, preferred_element_type=jnp.float32).astype(jnp.bfloat16)
    joined = joined.reshape(SEQ, HEADS, NOPE_DIM + VALUE_DIM).astype(jnp.float32)
    rotary = jnp.broadcast_to(rot_key.astype(jnp.float32)[:, None, :], (SEQ, HEADS, ROPE_DIM))
    key_full = jnp.concatenate([joined[:, :, :NOPE_DIM], rotary], axis=-1)
    values = joined[:, :, NOPE_DIM:]
    query_full = queries.astype(jnp.float32).reshape(SEQ, HEADS, head_dim)
    grad_full = out_grad.astype(jnp.float32).reshape(SEQ, HEADS, VALUE_DIM)
    row_delta = jnp.sum(outputs.astype(jnp.float32).reshape(SEQ, HEADS, VALUE_DIM) * grad_full, axis=-1)
    block_rows = math.gcd(SEQ, 512)
    block_count = SEQ // block_rows

    def block_step(totals, block_index):
        key_total, value_total = totals
        begin_row = (block_index * block_rows).astype(jnp.int32)
        query_block = lax.dynamic_slice_in_dim(query_full, begin_row, block_rows, 0)
        grad_block = lax.dynamic_slice_in_dim(grad_full, begin_row, block_rows, 0)
        log_block = lax.dynamic_slice_in_dim(log_sums, begin_row, block_rows, 0)
        delta_block = lax.dynamic_slice_in_dim(row_delta, begin_row, block_rows, 0)
        scores = jnp.einsum('qhd,khd->hqk', query_block, key_full) * score_scale
        probs = jnp.exp(scores - log_block.T[:, :, None])
        dprob = jnp.einsum('qhd,khd->hqk', grad_block, values)
        dscore = round_keep(probs * (dprob - delta_block.T[:, :, None]))
        probs_b = round_keep(probs)
        query_part = (jnp.einsum('hqk,khd->qhd', dscore, key_full) * score_scale).astype(jnp.bfloat16)
        key_total = key_total + jnp.einsum('hqk,qhd->khd', dscore, query_block) * score_scale
        value_total = value_total + jnp.einsum('hqk,qhd->khd', probs_b, grad_block)
        return (key_total, value_total), query_part

    start_totals = (jnp.zeros((SEQ, HEADS, head_dim), jnp.float32), jnp.zeros((SEQ, HEADS, VALUE_DIM), jnp.float32))
    (key_total, value_total), query_blocks = lax.scan(block_step, start_totals, jnp.arange(block_count, dtype=jnp.int32))
    query_grad = query_blocks.reshape(SEQ, HEADS * head_dim)
    rot_grad = jnp.sum(key_total[:, :, NOPE_DIM:], axis=1)
    key_grad = key_total[:, :, :NOPE_DIM].astype(jnp.bfloat16)
    value_grad = value_total.astype(jnp.bfloat16)
    stacked = jnp.concatenate([key_grad, value_grad], axis=-1).reshape(SEQ, HEADS * (NOPE_DIM + VALUE_DIM))
    weight_grad = jnp.dot(latents.T, stacked, preferred_element_type=jnp.float32)
    return (query_grad, key_grad.reshape(SEQ, HEADS * NOPE_DIM), value_grad.reshape(SEQ, HEADS * VALUE_DIM), rot_grad, weight_grad)
```

```python
import math

import jax
import jax.numpy as jnp
from jax import lax
from jax.experimental import pallas as pl
from jax.experimental.pallas import tpu as pltpu
from jax.sharding import Mesh, PartitionSpec as P

NOPE_DIM = 64
ROPE_DIM = 32
VALUE_DIM = 64
HEAD_DIM = NOPE_DIM + ROPE_DIM
SCALE = HEAD_DIM**-0.5
PAD = 16
Q_ROWS = HEAD_DIM + PAD + VALUE_DIM
K_ROWS = HEAD_DIM + VALUE_DIM
BF = jnp.bfloat16
F32 = jnp.float32

FAR = ("z3", "z2", "z1")
NEAR = ("z0", "y1", "y0")
HEADS_AXIS = ("x1", "x0", "c")
GROUP = 8
TOK = 128


def three_parts(row):
    high = row.astype(BF)
    rest = row - high.astype(F32)
    middle = rest.astype(BF)
    low = (rest - middle.astype(F32)).astype(BF)
    return high.astype(F32), middle.astype(F32), low.astype(F32)


def prepare_keys(latents, rot_key, weight, k_out):
    joined = lax.dot_general(
        latents[...], weight[...], (((1,), (0,)), ((), ())), preferred_element_type=F32
    )
    joined_t = joined.T.astype(BF)
    block = jnp.concatenate(
        [joined_t[:NOPE_DIM], rot_key[...], joined_t[NOPE_DIM:]], axis=0
    )
    for i in range(GROUP):
        k_out[i] = block


def prepare_queries(queries, logs, outputs, grads, q_out):
    q_t = queries[...].astype(F32)
    g_t = grads[...].astype(F32)
    o_t = outputs[...].astype(F32)
    delta = jnp.sum(o_t * g_t, axis=0, keepdims=True)
    rows = three_parts(logs[...] * (-1.0 / SCALE)) + three_parts(-delta)
    index = lax.broadcasted_iota(jnp.int32, (PAD, TOK), 0)
    pad = jnp.zeros((PAD, TOK), F32)
    for i, row in enumerate(rows):
        pad = jnp.where(index == i, row, pad)
    block = jnp.concatenate([q_t, pad, g_t], axis=0).astype(BF)
    for i in range(GROUP):
        q_out[i] = block


def attend(q_all, k_all, dq_out, dkv_out, q_t, q_tok, g_tok, k_t, k_tok, v_tok, dq_acc, dk_acc, dv_acc):
    total = GROUP * TOK
    lane = lax.broadcasted_iota(jnp.int32, (TOK, PAD), 1)
    key_pad = jnp.where(lane < 3, 1.0, 0.0).astype(F32)
    value_pad = jnp.where((lane >= 3) & (lane < 6), 1.0, 0.0).astype(F32)
    for i in range(GROUP):
        at = slice(i * TOK, (i + 1) * TOK)
        q_block = q_all[i]
        q_t[:, at] = q_block
        tok = q_block.astype(F32).T
        q_tok[at, :] = tok[:, :HEAD_DIM].astype(BF)
        g_tok[at, :] = tok[:, HEAD_DIM + PAD :].astype(BF)
        k_block = k_all[i]
        k_t[:, at] = k_block[:HEAD_DIM]
        ktok = k_block.astype(F32).T
        k_tok[at, :] = jnp.concatenate([ktok[:, :HEAD_DIM], key_pad], axis=1).astype(BF)
        v_tok[at, :] = jnp.concatenate([value_pad, ktok[:, HEAD_DIM:]], axis=1).astype(BF)
    step = 256
    for qi in range(total // step):
        qs = slice(qi * step, (qi + 1) * step)
        for ki in range(total // step):
            ks = slice(ki * step, (ki + 1) * step)
            scores = jnp.dot(k_tok[ks, :], q_t[: HEAD_DIM + PAD, qs], preferred_element_type=F32)
            probs = jnp.exp2(scores * (SCALE * math.log2(math.e)))
            dprob = jnp.dot(v_tok[ks, :], q_t[HEAD_DIM:, qs], preferred_element_type=F32)
            dscore = (probs * dprob).astype(BF)
            dk = jnp.dot(dscore, q_tok[qs, :], preferred_element_type=F32)
            dv = jnp.dot(probs.astype(BF), g_tok[qs, :], preferred_element_type=F32)
            dq = jnp.dot(k_t[:, ks], dscore, preferred_element_type=F32)
            if qi == 0:
                dk_acc[ks, :] = dk
                dv_acc[ks, :] = dv
            else:
                dk_acc[ks, :] += dk
                dv_acc[ks, :] += dv
            if ki == 0:
                dq_acc[:, qs] = dq
            else:
                dq_acc[:, qs] += dq
    for i in range(GROUP):
        at = slice(i * TOK, (i + 1) * TOK)
        dq_out[i] = (dq_acc[:, at] * SCALE).astype(BF)
        dkv_out[i] = jnp.concatenate(
            [(dk_acc[at, :] * SCALE).T, dv_acc[at, :].T], axis=0
        ).astype(BF)


def finish_keys(dkv, key_grad, value_grad, stacked_out, rot_out):
    total = dkv[0].astype(F32)
    for i in range(1, GROUP):
        total = total + dkv[i].astype(F32)
    rot = total[NOPE_DIM:HEAD_DIM]
    stacked_t = jnp.concatenate([total[:NOPE_DIM], total[HEAD_DIM:]], axis=0)
    stacked_out[...] = stacked_t.T.astype(BF)
    key_grad[...] = total[:NOPE_DIM].astype(BF)
    value_grad[...] = total[HEAD_DIM:].astype(BF)
    for i in range(GROUP):
        rot_out[i] = rot


def weigh(stacked, latents, weight_out):
    weight = lax.dot_general(
        latents[...], stacked[...], (((0,), (0,)), ((), ())), preferred_element_type=F32
    )
    by_owner = weight.reshape(GROUP, GROUP, 8, TOK)
    for i in range(GROUP):
        weight_out[i] = by_owner[:, i].reshape(GROUP * 8, TOK).astype(BF)


def join_far(weight, dq, far_out):
    total = weight[0].astype(F32)
    for i in range(1, GROUP):
        total = total + weight[i].astype(F32)
    for i in range(GROUP):
        rows = total[i * 8 : (i + 1) * 8]
        high = rows.astype(BF).astype(F32)
        far_out[i, :HEAD_DIM] = dq[i]
        far_out[i, HEAD_DIM:] = jnp.concatenate([high, rows - high], axis=0).astype(BF)


def finish_rest(far, rot, query_grad, weight_grad, rot_grad):
    total = far[0].astype(F32)
    around = rot[0]
    for i in range(1, GROUP):
        total = total + far[i].astype(F32)
        around = around + rot[i]
    query_grad[...] = total[:HEAD_DIM].astype(BF)
    weight_grad[...] = total[HEAD_DIM : HEAD_DIM + 8] + total[HEAD_DIM + 8 :]
    rot_grad[...] = around


def call(body, args, outs, name, scratch=()):
    shapes = [
        pltpu.VMEM(shape, kind) if near else jax.ShapeDtypeStruct(shape, kind)
        for shape, kind, near in outs
    ]
    return pl.pallas_call(body, out_shape=shapes, scratch_shapes=list(scratch), name=name)(*args)


def close(x):
    return pltpu.with_memory_space_constraint(x, pltpu.VMEM)


def exchange(x, axes):
    return close(lax.all_to_all(x, axes, split_axis=0, concat_axis=0, tiled=True))


def per_device(queries, latents, rot_key, kv_weight, log_sums, outputs, out_grad):
    total = GROUP * TOK
    (k_send,) = call(
        prepare_keys,
        (latents, rot_key.T, kv_weight),
        [((GROUP, K_ROWS, TOK), BF, True)],
        "prepare_keys",
    )
    (q_send,) = call(
        prepare_queries,
        (queries.T, log_sums.T, outputs.T, out_grad.T),
        [((GROUP, Q_ROWS, TOK), BF, True)],
        "prepare_queries",
    )
    k_all = exchange(k_send, NEAR)
    q_all = exchange(q_send, FAR)
    dq, dkv = call(
        attend,
        (q_all, k_all),
        [((GROUP, HEAD_DIM, TOK), BF, True), ((GROUP, K_ROWS, TOK), BF, True)],
        "attend",
        [
            pltpu.VMEM((Q_ROWS, total), BF),
            pltpu.VMEM((total, HEAD_DIM), BF),
            pltpu.VMEM((total, VALUE_DIM), BF),
            pltpu.VMEM((HEAD_DIM, total), BF),
            pltpu.VMEM((total, HEAD_DIM + PAD), BF),
            pltpu.VMEM((total, PAD + VALUE_DIM), BF),
            pltpu.VMEM((HEAD_DIM, total), F32),
            pltpu.VMEM((total, HEAD_DIM), F32),
            pltpu.VMEM((total, VALUE_DIM), F32),
        ],
    )
    key_grad, value_grad, stacked, rot_send = call(
        finish_keys,
        (exchange(dkv, NEAR),),
        [
            ((NOPE_DIM, TOK), BF, False),
            ((VALUE_DIM, TOK), BF, False),
            ((TOK, NOPE_DIM + VALUE_DIM), BF, True),
            ((GROUP, ROPE_DIM, TOK), F32, True),
        ],
        "finish_keys",
    )
    rot_all = exchange(rot_send, HEADS_AXIS)
    (weight_send,) = call(
        weigh, (close(stacked), latents), [((GROUP, GROUP * 8, TOK), BF, True)], "weigh"
    )
    (far_send,) = call(
        join_far,
        (exchange(weight_send, NEAR), close(dq)),
        [((GROUP, HEAD_DIM + 16, TOK), BF, True)],
        "join_far",
    )
    query_grad, weight_grad, rot_grad = call(
        finish_rest,
        (exchange(far_send, FAR), rot_all),
        [((HEAD_DIM, TOK), BF, False), ((8, TOK), F32, False), ((ROPE_DIM, TOK), F32, False)],
        "finish_rest",
    )
    return query_grad.T, key_grad.T, value_grad.T, rot_grad.T, weight_grad


def solution(mesh):
    sp, tp = FAR + NEAR, HEADS_AXIS
    split = Mesh(mesh.devices.reshape((2,) * 9), sp + tp)
    placed = (P(sp, tp), P(sp, None), P(sp, None), P(None, tp), P(sp, tp), P(sp, tp), P(sp, tp))
    return jax.shard_map(
        per_device,
        mesh=split,
        in_specs=placed,
        out_specs=(P(sp, tp), P(sp, tp), P(sp, tp), P(sp, None), P(sp, tp)),
        check_vma=False,
    )
```

```python
import math

import jax
import jax.numpy as jnp
from jax import lax
from jax.experimental import pallas as pl
from jax.experimental.pallas import tpu as pltpu
from jax.sharding import Mesh, PartitionSpec as P

NOPE_DIM = 64
ROPE_DIM = 32
VALUE_DIM = 64
HEAD_DIM = NOPE_DIM + ROPE_DIM
SCALE = HEAD_DIM**-0.5
PAD = 16
Q_ROWS = HEAD_DIM + PAD + VALUE_DIM
K_ROWS = HEAD_DIM + VALUE_DIM
BF = jnp.bfloat16
F32 = jnp.float32

FAR = ("z3", "z2", "z1")
NEAR = ("y1", "y0", "z0")
HEADS_AXIS = ("x1", "x0", "c")
GROUP = 8
TOK = 128


def three_parts(row):
    high = row.astype(BF)
    rest = row - high.astype(F32)
    middle = rest.astype(BF)
    low = (rest - middle.astype(F32)).astype(BF)
    return high.astype(F32), middle.astype(F32), low.astype(F32)


def prepare_keys(latents, rot_key, weight, k_out):
    joined = lax.dot_general(
        latents[...], weight[...], (((1,), (0,)), ((), ())), preferred_element_type=F32
    )
    joined_t = joined.T.astype(BF)
    block = jnp.concatenate(
        [joined_t[:NOPE_DIM], rot_key[...], joined_t[NOPE_DIM:]], axis=0
    )
    k_out[...] = block


def prepare_queries(queries, logs, outputs, grads, q_out):
    q_t = queries[...].astype(F32)
    g_t = grads[...].astype(F32)
    o_t = outputs[...].astype(F32)
    delta = jnp.sum(o_t * g_t, axis=0, keepdims=True)
    rows = three_parts(logs[...] * (-1.0 / SCALE)) + three_parts(-delta)
    index = lax.broadcasted_iota(jnp.int32, (PAD, TOK), 0)
    pad = jnp.zeros((PAD, TOK), F32)
    for i, row in enumerate(rows):
        pad = jnp.where(index == i, row, pad)
    block = jnp.concatenate([q_t, pad, g_t], axis=0).astype(BF)
    for i in range(GROUP):
        q_out[i] = block


def attend(q_all, k_all, dq_out, dkv_out, q_t, q_tok, g_tok, k_t, k_tok, v_tok, dq_acc, dk_acc, dv_acc):
    total = GROUP * TOK
    lane = lax.broadcasted_iota(jnp.int32, (TOK, PAD), 1)
    key_pad = jnp.where(lane < 3, 1.0, 0.0).astype(F32)
    value_pad = jnp.where((lane >= 3) & (lane < 6), 1.0, 0.0).astype(F32)
    for i in range(GROUP):
        at = slice(i * TOK, (i + 1) * TOK)
        q_block = q_all[i]
        q_t[:, at] = q_block
        tok = q_block.astype(F32).T
        q_tok[at, :] = tok[:, :HEAD_DIM].astype(BF)
        g_tok[at, :] = tok[:, HEAD_DIM + PAD :].astype(BF)
        k_block = k_all[i]
        k_t[:, at] = k_block[:HEAD_DIM]
        ktok = k_block.astype(F32).T
        k_tok[at, :] = jnp.concatenate([ktok[:, :HEAD_DIM], key_pad], axis=1).astype(BF)
        v_tok[at, :] = jnp.concatenate([value_pad, ktok[:, HEAD_DIM:]], axis=1).astype(BF)
    step = 256
    for qi in range(total // step):
        qs = slice(qi * step, (qi + 1) * step)
        for ki in range(total // step):
            ks = slice(ki * step, (ki + 1) * step)
            scores = jnp.dot(k_tok[ks, :], q_t[: HEAD_DIM + PAD, qs], preferred_element_type=F32)
            probs = jnp.exp2(scores * (SCALE * math.log2(math.e)))
            dprob = jnp.dot(v_tok[ks, :], q_t[HEAD_DIM:, qs], preferred_element_type=F32)
            dscore = (probs * dprob).astype(BF)
            dk = jnp.dot(dscore, q_tok[qs, :], preferred_element_type=F32)
            dv = jnp.dot(probs.astype(BF), g_tok[qs, :], preferred_element_type=F32)
            dq = jnp.dot(k_t[:, ks], dscore, preferred_element_type=F32)
            if qi == 0:
                dk_acc[ks, :] = dk
                dv_acc[ks, :] = dv
            else:
                dk_acc[ks, :] += dk
                dv_acc[ks, :] += dv
            if ki == 0:
                dq_acc[:, qs] = dq
            else:
                dq_acc[:, qs] += dq
    for i in range(GROUP):
        at = slice(i * TOK, (i + 1) * TOK)
        dq_out[i] = (dq_acc[:, at] * SCALE).astype(BF)
        dkv_out[i] = jnp.concatenate(
            [(dk_acc[at, :] * SCALE).T, dv_acc[at, :].T], axis=0
        ).astype(BF)


def finish_keys(dkv, key_grad, value_grad, stacked_out, rot_out):
    total = dkv[0].astype(F32)
    for i in range(1, GROUP):
        total = total + dkv[i].astype(F32)
    rot = total[NOPE_DIM:HEAD_DIM]
    stacked_t = jnp.concatenate([total[:NOPE_DIM], total[HEAD_DIM:]], axis=0)
    stacked_out[...] = stacked_t.T.astype(BF)
    key_grad[...] = total[:NOPE_DIM].astype(BF)
    value_grad[...] = total[HEAD_DIM:].astype(BF)
    rot_out[...] = rot


def weigh(stacked, latents, weight_out):
    weight = lax.dot_general(
        latents[...], stacked[...], (((0,), (0,)), ((), ())), preferred_element_type=F32
    )
    by_owner = weight.reshape(GROUP, GROUP, 8, TOK)
    for i in range(GROUP):
        owner = (i % 2) * 4 + i // 2
        weight_out[i] = by_owner[:, owner].reshape(GROUP * 8, TOK).astype(BF)


def join_far(weight, dq, far_out):
    total = weight[0].astype(F32)
    for i in range(1, GROUP):
        total = total + weight[i].astype(F32)
    for i in range(GROUP):
        rows = total[i * 8 : (i + 1) * 8]
        high = rows.astype(BF).astype(F32)
        far_out[i, :HEAD_DIM] = dq[i]
        far_out[i, HEAD_DIM:] = jnp.concatenate([high, rows - high], axis=0).astype(BF)


def finish_rest(far, rot, query_grad, weight_grad, rot_grad):
    total = far[0].astype(F32)
    around = rot[0]
    for i in range(1, GROUP):
        total = total + far[i].astype(F32)
        around = around + rot[i]
    query_grad[...] = total[:HEAD_DIM].astype(BF)
    weight_grad[...] = total[HEAD_DIM : HEAD_DIM + 8] + total[HEAD_DIM + 8 :]
    rot_grad[...] = around


def call(body, args, outs, name, scratch=()):
    shapes = [
        pltpu.VMEM(shape, kind) if near else jax.ShapeDtypeStruct(shape, kind)
        for shape, kind, near in outs
    ]
    return pl.pallas_call(body, out_shape=shapes, scratch_shapes=list(scratch), name=name)(*args)


def close(x):
    return pltpu.with_memory_space_constraint(x, pltpu.VMEM)


def exchange(x, axes):
    return close(lax.all_to_all(x, axes, split_axis=0, concat_axis=0, tiled=True))


def gather_pairs(x, axes):
    for axis in axes:
        x = lax.all_gather(x, axis, axis=0)
    return close(x.reshape((GROUP,) + x.shape[len(axes) :]))


def per_device(queries, latents, rot_key, kv_weight, log_sums, outputs, out_grad):
    total = GROUP * TOK
    (k_send,) = call(
        prepare_keys,
        (latents, rot_key.T, kv_weight),
        [((K_ROWS, TOK), BF, True)],
        "prepare_keys",
    )
    (q_send,) = call(
        prepare_queries,
        (queries.T, log_sums.T, outputs.T, out_grad.T),
        [((GROUP, Q_ROWS, TOK), BF, True)],
        "prepare_queries",
    )
    k_all = gather_pairs(k_send, NEAR[::-1])
    q_all = exchange(q_send, FAR)
    dq, dkv = call(
        attend,
        (q_all, k_all),
        [((GROUP, HEAD_DIM, TOK), BF, True), ((GROUP, K_ROWS, TOK), BF, True)],
        "attend",
        [
            pltpu.VMEM((Q_ROWS, total), BF),
            pltpu.VMEM((total, HEAD_DIM), BF),
            pltpu.VMEM((total, VALUE_DIM), BF),
            pltpu.VMEM((HEAD_DIM, total), BF),
            pltpu.VMEM((total, HEAD_DIM + PAD), BF),
            pltpu.VMEM((total, PAD + VALUE_DIM), BF),
            pltpu.VMEM((HEAD_DIM, total), F32),
            pltpu.VMEM((total, HEAD_DIM), F32),
            pltpu.VMEM((total, VALUE_DIM), F32),
        ],
    )
    key_grad, value_grad, stacked, rot_send = call(
        finish_keys,
        (exchange(dkv, NEAR),),
        [
            ((NOPE_DIM, TOK), BF, False),
            ((VALUE_DIM, TOK), BF, False),
            ((TOK, NOPE_DIM + VALUE_DIM), BF, True),
            ((ROPE_DIM, TOK), F32, True),
        ],
        "finish_keys",
    )
    rot_all = gather_pairs(rot_send, HEADS_AXIS[::-1])
    (weight_send,) = call(
        weigh, (close(stacked), latents), [((GROUP, GROUP * 8, TOK), BF, True)], "weigh"
    )
    (far_send,) = call(
        join_far,
        (exchange(weight_send, NEAR), close(dq)),
        [((GROUP, HEAD_DIM + 16, TOK), BF, True)],
        "join_far",
    )
    query_grad, weight_grad, rot_grad = call(
        finish_rest,
        (exchange(far_send, FAR), rot_all),
        [((HEAD_DIM, TOK), BF, False), ((8, TOK), F32, False), ((ROPE_DIM, TOK), F32, False)],
        "finish_rest",
    )
    return query_grad.T, key_grad.T, value_grad.T, rot_grad.T, weight_grad


def solution(mesh):
    sp, tp = FAR + ("z0", "y1", "y0"), HEADS_AXIS
    split = Mesh(mesh.devices.reshape((2,) * 9), sp + tp)
    placed = (P(sp, tp), P(sp, None), P(sp, None), P(None, tp), P(sp, tp), P(sp, tp), P(sp, tp))
    return jax.shard_map(
        per_device,
        mesh=split,
        in_specs=placed,
        out_specs=(P(sp, tp), P(sp, tp), P(sp, tp), P(sp, None), P(sp, tp)),
        check_vma=False,
    )
```

```python
import math

import jax
import jax.numpy as jnp
from jax import lax
from jax.experimental import pallas as pl
from jax.experimental.pallas import tpu as pltpu
from jax.sharding import Mesh, PartitionSpec as P

NOPE_DIM = 64
ROPE_DIM = 32
VALUE_DIM = 64
HEAD_DIM = NOPE_DIM + ROPE_DIM
SCALE = HEAD_DIM**-0.5
PAD = 16
Q_ROWS = HEAD_DIM + PAD + VALUE_DIM
K_ROWS = HEAD_DIM + VALUE_DIM
BF = jnp.bfloat16
F32 = jnp.float32

FAR = ("z3", "z2", "z1")
NEAR = ("z0", "y1", "y0")
HEADS_AXIS = ("x1", "x0", "c")
GROUP = 8
TOK = 128


def three_parts(row):
    high = row.astype(BF)
    rest = row - high.astype(F32)
    middle = rest.astype(BF)
    low = (rest - middle.astype(F32)).astype(BF)
    return high.astype(F32), middle.astype(F32), low.astype(F32)


def prepare_keys(latents, rot_key, weight, k_out):
    joined = lax.dot_general(
        latents[...], weight[...], (((1,), (0,)), ((), ())), preferred_element_type=F32
    )
    joined_t = joined.T.astype(BF)
    block = jnp.concatenate(
        [joined_t[:NOPE_DIM], rot_key[...], joined_t[NOPE_DIM:]], axis=0
    )
    k_out[...] = block


def prepare_queries(queries, logs, outputs, grads, q_out):
    q_t = queries[...].astype(F32)
    g_t = grads[...].astype(F32)
    o_t = outputs[...].astype(F32)
    delta = jnp.sum(o_t * g_t, axis=0, keepdims=True)
    rows = three_parts(logs[...] * (-1.0 / SCALE)) + three_parts(-delta)
    index = lax.broadcasted_iota(jnp.int32, (PAD, TOK), 0)
    pad = jnp.zeros((PAD, TOK), F32)
    for i, row in enumerate(rows):
        pad = jnp.where(index == i, row, pad)
    block = jnp.concatenate([q_t, pad, g_t], axis=0).astype(BF)
    for i in range(GROUP):
        q_out[i] = block


def attend(q_all, k_all, dq_out, dkv_out, q_t, q_tok, g_tok, k_t, k_tok, v_tok, dq_acc, dk_acc, dv_acc, dscores, probs_b):
    total = GROUP * TOK
    lane = lax.broadcasted_iota(jnp.int32, (TOK, PAD), 1)
    key_pad = jnp.where(lane < 3, 1.0, 0.0).astype(F32)
    value_pad = jnp.where((lane >= 3) & (lane < 6), 1.0, 0.0).astype(F32)
    for i in range(GROUP):
        at = slice(i * TOK, (i + 1) * TOK)
        q_block = q_all[i]
        q_t[:, at] = q_block
        tok = q_block.astype(F32).T
        q_tok[at, :] = tok[:, :HEAD_DIM].astype(BF)
        g_tok[at, :] = tok[:, HEAD_DIM + PAD :].astype(BF)
        k_block = k_all[i]
        k_t[:, at] = k_block[:HEAD_DIM]
        ktok = k_block.astype(F32).T
        k_tok[at, :] = jnp.concatenate([ktok[:, :HEAD_DIM], key_pad], axis=1).astype(BF)
        v_tok[at, :] = jnp.concatenate([value_pad, ktok[:, HEAD_DIM:]], axis=1).astype(BF)
    step = 256
    for ki in range(total // step):
        ks = slice(ki * step, (ki + 1) * step)
        for qi in range(total // step):
            qs = slice(qi * step, (qi + 1) * step)
            scores = jnp.dot(k_tok[ks, :], q_t[: HEAD_DIM + PAD, qs], preferred_element_type=F32)
            probs = jnp.exp2(scores * (SCALE * math.log2(math.e)))
            dprob = jnp.dot(v_tok[ks, :], q_t[HEAD_DIM:, qs], preferred_element_type=F32)
            dscores[ks, qs] = (probs * dprob).astype(BF)
            probs_b[ks, qs] = probs.astype(BF)
        dk_acc[ks, :] = jnp.dot(dscores[ks, :], q_tok[...], preferred_element_type=F32)
        dv_acc[ks, :] = jnp.dot(probs_b[ks, :], g_tok[...], preferred_element_type=F32)
    for qi in range(total // step):
        qs = slice(qi * step, (qi + 1) * step)
        dq_acc[:, qs] = jnp.dot(k_t[...], dscores[:, qs], preferred_element_type=F32)
    for i in range(GROUP):
        at = slice(i * TOK, (i + 1) * TOK)
        dq_out[i] = (dq_acc[:, at] * SCALE).astype(BF)
        dkv_out[i] = jnp.concatenate(
            [(dk_acc[at, :] * SCALE).T, dv_acc[at, :].T], axis=0
        ).astype(BF)


def finish_keys(dkv, latents, key_grad, value_grad, rot_out, weight_out):
    total = dkv[0].astype(F32)
    for i in range(1, GROUP):
        total = total + dkv[i].astype(F32)
    rot_out[...] = total[NOPE_DIM:HEAD_DIM]
    key_grad[...] = total[:NOPE_DIM].astype(BF)
    value_grad[...] = total[HEAD_DIM:].astype(BF)
    stacked = jnp.concatenate([total[:NOPE_DIM], total[HEAD_DIM:]], axis=0).T.astype(BF)
    weight = lax.dot_general(
        latents[...], stacked, (((0,), (0,)), ((), ())), preferred_element_type=F32
    )
    by_owner = weight.reshape(GROUP, GROUP, 8, TOK)
    for i in range(GROUP):
        weight_out[i] = by_owner[:, i].reshape(GROUP * 8, TOK).astype(BF)


def join_far(weight, dq, far_out):
    total = weight[0].astype(F32)
    for i in range(1, GROUP):
        total = total + weight[i].astype(F32)
    for i in range(GROUP):
        rows = total[i * 8 : (i + 1) * 8]
        high = rows.astype(BF).astype(F32)
        far_out[i, :HEAD_DIM] = dq[i]
        far_out[i, HEAD_DIM:] = jnp.concatenate([high, rows - high], axis=0).astype(BF)


def finish_rest(far, rot, query_grad, weight_grad, rot_grad):
    total = far[0].astype(F32)
    around = rot[0]
    for i in range(1, GROUP):
        total = total + far[i].astype(F32)
        around = around + rot[i]
    query_grad[...] = total[:HEAD_DIM].astype(BF)
    weight_grad[...] = total[HEAD_DIM : HEAD_DIM + 8] + total[HEAD_DIM + 8 :]
    rot_grad[...] = around


def call(body, args, outs, name, scratch=()):
    shapes = [
        pltpu.VMEM(shape, kind) if near else jax.ShapeDtypeStruct(shape, kind)
        for shape, kind, near in outs
    ]
    return pl.pallas_call(body, out_shape=shapes, scratch_shapes=list(scratch), name=name)(*args)


def close(x):
    return pltpu.with_memory_space_constraint(x, pltpu.VMEM)


def exchange(x, axes):
    return close(lax.all_to_all(x, axes, split_axis=0, concat_axis=0, tiled=True))


def gather_pairs(x, axes):
    for axis in axes:
        x = lax.all_gather(x, axis, axis=0)
    return close(x.reshape((GROUP,) + x.shape[len(axes) :]))


def per_device(queries, latents, rot_key, kv_weight, log_sums, outputs, out_grad):
    total = GROUP * TOK
    (k_send,) = call(
        prepare_keys,
        (latents, rot_key.T, kv_weight),
        [((K_ROWS, TOK), BF, True)],
        "prepare_keys",
    )
    (q_send,) = call(
        prepare_queries,
        (queries.T, log_sums.T, outputs.T, out_grad.T),
        [((GROUP, Q_ROWS, TOK), BF, True)],
        "prepare_queries",
    )
    k_all = gather_pairs(k_send, NEAR[::-1])
    q_all = exchange(q_send, FAR)
    dq, dkv = call(
        attend,
        (q_all, k_all),
        [((GROUP, HEAD_DIM, TOK), BF, True), ((GROUP, K_ROWS, TOK), BF, True)],
        "attend",
        [
            pltpu.VMEM((Q_ROWS, total), BF),
            pltpu.VMEM((total, HEAD_DIM), BF),
            pltpu.VMEM((total, VALUE_DIM), BF),
            pltpu.VMEM((HEAD_DIM, total), BF),
            pltpu.VMEM((total, HEAD_DIM + PAD), BF),
            pltpu.VMEM((total, PAD + VALUE_DIM), BF),
            pltpu.VMEM((HEAD_DIM, total), F32),
            pltpu.VMEM((total, HEAD_DIM), F32),
            pltpu.VMEM((total, VALUE_DIM), F32),
            pltpu.VMEM((total, total), BF),
            pltpu.VMEM((total, total), BF),
        ],
    )
    key_grad, value_grad, rot_send, weight_send = call(
        finish_keys,
        (exchange(dkv, NEAR), latents),
        [
            ((NOPE_DIM, TOK), BF, False),
            ((VALUE_DIM, TOK), BF, False),
            ((ROPE_DIM, TOK), F32, True),
            ((GROUP, GROUP * 8, TOK), BF, True),
        ],
        "finish_keys",
    )
    rot_all = gather_pairs(rot_send, HEADS_AXIS[::-1])
    (far_send,) = call(
        join_far,
        (exchange(weight_send, NEAR), close(dq)),
        [((GROUP, HEAD_DIM + 16, TOK), BF, True)],
        "join_far",
    )
    query_grad, weight_grad, rot_grad = call(
        finish_rest,
        (exchange(far_send, FAR), rot_all),
        [((HEAD_DIM, TOK), BF, False), ((8, TOK), F32, False), ((ROPE_DIM, TOK), F32, False)],
        "finish_rest",
    )
    return query_grad.T, key_grad.T, value_grad.T, rot_grad.T, weight_grad


def solution(mesh):
    sp, tp = FAR + NEAR, HEADS_AXIS
    split = Mesh(mesh.devices.reshape((2,) * 9), sp + tp)
    placed = (P(sp, tp), P(sp, None), P(sp, None), P(None, tp), P(sp, tp), P(sp, tp), P(sp, tp))
    return jax.shard_map(
        per_device,
        mesh=split,
        in_specs=placed,
        out_specs=(P(sp, tp), P(sp, tp), P(sp, tp), P(sp, None), P(sp, tp)),
        check_vma=False,
    )
```

```python
import math

import jax
import jax.numpy as jnp
from jax import lax
from jax.experimental import pallas as pl
from jax.experimental.pallas import tpu as pltpu
from jax.sharding import Mesh, PartitionSpec as P

NOPE_DIM = 64
ROPE_DIM = 32
VALUE_DIM = 64
HEAD_DIM = NOPE_DIM + ROPE_DIM
SCALE = HEAD_DIM**-0.5
PAD = 16
Q_ROWS = HEAD_DIM + PAD + VALUE_DIM
K_ROWS = HEAD_DIM + VALUE_DIM
BF = jnp.bfloat16
F32 = jnp.float32

FAR = ("z3", "z2", "z1")
NEAR = ("z0", "y1", "y0")
HEADS_AXIS = ("x1", "x0", "c")
GROUP = 8
TOK = 128


def three_parts(row):
    high = row.astype(BF)
    rest = row - high.astype(F32)
    middle = rest.astype(BF)
    low = (rest - middle.astype(F32)).astype(BF)
    return high.astype(F32), middle.astype(F32), low.astype(F32)


def prepare(latents, rot_key, weight, queries, logs, outputs, grads, k_out, q_out):
    joined = lax.dot_general(
        latents[...], weight[...], (((1,), (0,)), ((), ())), preferred_element_type=F32
    )
    joined_t = joined.T.astype(BF)
    k_out[:NOPE_DIM] = joined_t[:NOPE_DIM]
    k_out[NOPE_DIM:HEAD_DIM] = rot_key[...]
    k_out[HEAD_DIM:] = joined_t[NOPE_DIM:]
    q_t = queries[...].astype(F32)
    g_t = grads[...].astype(F32)
    delta = jnp.sum(outputs[...].astype(F32) * g_t, axis=0, keepdims=True)
    rows = three_parts(logs[...] * (-1.0 / SCALE)) + three_parts(-delta)
    index = lax.broadcasted_iota(jnp.int32, (PAD, TOK), 0)
    pad = jnp.zeros((PAD, TOK), F32)
    for i, row in enumerate(rows):
        pad = jnp.where(index == i, row, pad)
    block = jnp.concatenate([q_t, pad, g_t], axis=0).astype(BF)
    for i in range(GROUP):
        q_out[i] = block


def attend(q_all, k_all, dq_out, dkv_out, q_t, q_tok, g_tok, k_t, k_tok, v_tok, dq_acc, dk_acc, dv_acc, dscores, probs_b):
    total = GROUP * TOK
    lane = lax.broadcasted_iota(jnp.int32, (TOK, PAD), 1)
    key_pad = jnp.where(lane < 3, 1.0, 0.0).astype(F32)
    value_pad = jnp.where((lane >= 3) & (lane < 6), 1.0, 0.0).astype(F32)
    for i in range(GROUP):
        at = slice(i * TOK, (i + 1) * TOK)
        q_block = q_all[i]
        q_t[:, at] = q_block
        tok = q_block.astype(F32).T
        q_tok[at, :] = tok[:, :HEAD_DIM].astype(BF)
        g_tok[at, :] = tok[:, HEAD_DIM + PAD :].astype(BF)
        k_block = k_all[(i % 4) * 2 + i // 4]
        k_t[:, at] = k_block[:HEAD_DIM]
        ktok = k_block.astype(F32).T
        k_tok[at, :] = jnp.concatenate([ktok[:, :HEAD_DIM], key_pad], axis=1).astype(BF)
        v_tok[at, :] = jnp.concatenate([value_pad, ktok[:, HEAD_DIM:]], axis=1).astype(BF)
    step = 256
    for ki in range(total // step):
        ks = slice(ki * step, (ki + 1) * step)
        for qi in range(total // step):
            qs = slice(qi * step, (qi + 1) * step)
            scores = jnp.dot(k_tok[ks, :], q_t[: HEAD_DIM + PAD, qs], preferred_element_type=F32)
            probs = jnp.exp2(scores * (SCALE * math.log2(math.e)))
            dprob = jnp.dot(v_tok[ks, :], q_t[HEAD_DIM:, qs], preferred_element_type=F32)
            dscores[ks, qs] = (probs * dprob).astype(BF)
            probs_b[ks, qs] = probs.astype(BF)
        dk_acc[ks, :] = jnp.dot(dscores[ks, :], q_tok[...], preferred_element_type=F32)
        dv_acc[ks, :] = jnp.dot(probs_b[ks, :], g_tok[...], preferred_element_type=F32)
    for qi in range(total // step):
        qs = slice(qi * step, (qi + 1) * step)
        dq_acc[:, qs] = jnp.dot(k_t[...], dscores[:, qs], preferred_element_type=F32)
    for i in range(GROUP):
        at = slice(i * TOK, (i + 1) * TOK)
        dq_out[i] = (dq_acc[:, at] * SCALE).astype(BF)
        dkv_out[i] = jnp.concatenate(
            [(dk_acc[at, :] * SCALE).T, dv_acc[at, :].T], axis=0
        ).astype(BF)


def finish_keys(dkv, latents, key_grad, value_grad, rot_out, weight_out):
    total = dkv[0].astype(F32)
    for i in range(1, GROUP):
        total = total + dkv[i].astype(F32)
    rot_out[...] = total[NOPE_DIM:HEAD_DIM]
    key_grad[...] = total[:NOPE_DIM].astype(BF)
    value_grad[...] = total[HEAD_DIM:].astype(BF)
    stacked = jnp.concatenate([total[:NOPE_DIM], total[HEAD_DIM:]], axis=0).T.astype(BF)
    weight = lax.dot_general(
        latents[...], stacked, (((0,), (0,)), ((), ())), preferred_element_type=F32
    )
    by_owner = weight.reshape(GROUP, GROUP, 8, TOK)
    for i in range(GROUP):
        weight_out[i] = by_owner[:, i].reshape(GROUP * 8, TOK).astype(BF)


def join_far(weight, dq, far_out):
    total = weight[0].astype(F32)
    for i in range(1, GROUP):
        total = total + weight[i].astype(F32)
    for i in range(GROUP):
        rows = total[i * 8 : (i + 1) * 8]
        high = rows.astype(BF).astype(F32)
        far_out[i, :HEAD_DIM] = dq[i]
        far_out[i, HEAD_DIM:] = jnp.concatenate([high, rows - high], axis=0).astype(BF)


def finish_rest(far, rot, query_grad, weight_grad, rot_grad):
    total = far[0].astype(F32)
    around = rot[0]
    for i in range(1, GROUP):
        total = total + far[i].astype(F32)
        around = around + rot[i]
    query_grad[...] = total[:HEAD_DIM].astype(BF)
    weight_grad[...] = total[HEAD_DIM : HEAD_DIM + 8] + total[HEAD_DIM + 8 :]
    rot_grad[...] = around


def call(body, args, outs, name, scratch=()):
    shapes = [
        pltpu.VMEM(shape, kind) if near else jax.ShapeDtypeStruct(shape, kind)
        for shape, kind, near in outs
    ]
    return pl.pallas_call(body, out_shape=shapes, scratch_shapes=list(scratch), name=name)(*args)


def close(x):
    return pltpu.with_memory_space_constraint(x, pltpu.VMEM)


def exchange(x, axes):
    return close(lax.all_to_all(x, axes, split_axis=0, concat_axis=0, tiled=True))


def gather_pairs(x, axes):
    for axis in axes:
        x = lax.all_gather(x, axis, axis=0)
    return x


def per_device(queries, latents, rot_key, kv_weight, log_sums, outputs, out_grad):
    total = GROUP * TOK
    k_send, q_send = call(
        prepare,
        (latents, rot_key.T, kv_weight, queries.T, log_sums.T, outputs.T, out_grad.T),
        [((K_ROWS, TOK), BF, True), ((GROUP, Q_ROWS, TOK), BF, False)],
        "prepare",
    )
    k_pair = gather_pairs(k_send, ("z0",))
    q_send, k_pair = lax.optimization_barrier((q_send, k_pair))
    q_all = exchange(q_send, FAR)
    k_all = close(gather_pairs(k_pair, ("y0", "y1")).reshape(GROUP, K_ROWS, TOK))
    dq, dkv = call(
        attend,
        (q_all, k_all),
        [((GROUP, HEAD_DIM, TOK), BF, True), ((GROUP, K_ROWS, TOK), BF, True)],
        "attend",
        [
            pltpu.VMEM((Q_ROWS, total), BF),
            pltpu.VMEM((total, HEAD_DIM), BF),
            pltpu.VMEM((total, VALUE_DIM), BF),
            pltpu.VMEM((HEAD_DIM, total), BF),
            pltpu.VMEM((total, HEAD_DIM + PAD), BF),
            pltpu.VMEM((total, PAD + VALUE_DIM), BF),
            pltpu.VMEM((HEAD_DIM, total), F32),
            pltpu.VMEM((total, HEAD_DIM), F32),
            pltpu.VMEM((total, VALUE_DIM), F32),
            pltpu.VMEM((total, total), BF),
            pltpu.VMEM((total, total), BF),
        ],
    )
    key_grad, value_grad, rot_send, weight_send = call(
        finish_keys,
        (exchange(dkv, NEAR), latents),
        [
            ((NOPE_DIM, TOK), BF, False),
            ((VALUE_DIM, TOK), BF, False),
            ((ROPE_DIM, TOK), F32, True),
            ((GROUP, GROUP * 8, TOK), BF, True),
        ],
        "finish_keys",
    )
    rot_all = close(gather_pairs(rot_send, HEADS_AXIS[::-1]).reshape(GROUP, ROPE_DIM, TOK))
    (far_send,) = call(
        join_far,
        (exchange(weight_send, NEAR), close(dq)),
        [((GROUP, HEAD_DIM + 16, TOK), BF, True)],
        "join_far",
    )
    query_grad, weight_grad, rot_grad = call(
        finish_rest,
        (exchange(far_send, FAR), rot_all),
        [((HEAD_DIM, TOK), BF, False), ((8, TOK), F32, False), ((ROPE_DIM, TOK), F32, False)],
        "finish_rest",
    )
    return query_grad.T, key_grad.T, value_grad.T, rot_grad.T, weight_grad


def solution(mesh):
    sp, tp = FAR + NEAR, HEADS_AXIS
    split = Mesh(mesh.devices.reshape((2,) * 9), sp + tp)
    placed = (P(sp, tp), P(sp, None), P(sp, None), P(None, tp), P(sp, tp), P(sp, tp), P(sp, tp))
    return jax.shard_map(
        per_device,
        mesh=split,
        in_specs=placed,
        out_specs=(P(sp, tp), P(sp, tp), P(sp, tp), P(sp, None), P(sp, tp)),
        check_vma=False,
    )
```

```python
import math

import jax
import jax.numpy as jnp
from jax import lax
from jax.experimental import pallas as pl
from jax.experimental.pallas import tpu as pltpu
from jax.sharding import Mesh, PartitionSpec as P

NOPE_DIM = 64
ROPE_DIM = 32
VALUE_DIM = 64
HEAD_DIM = NOPE_DIM + ROPE_DIM
SCALE = HEAD_DIM**-0.5
PAD = 8
FAR_ROWS = HEAD_DIM + 8
Q_ROWS = HEAD_DIM + PAD + VALUE_DIM
K_ROWS = HEAD_DIM + VALUE_DIM
BF = jnp.bfloat16
F32 = jnp.float32

FAR = ("z3", "z2", "z1")
NEAR = ("z0", "y1", "y0")
HEADS_AXIS = ("x1", "x0", "c")
GROUP = 8
TOK = 128


def three_parts(row):
    high = row.astype(BF)
    rest = row - high.astype(F32)
    middle = rest.astype(BF)
    low = (rest - middle.astype(F32)).astype(BF)
    return high.astype(F32), middle.astype(F32), low.astype(F32)


def prepare(latents, rot_key, weight, queries, logs, outputs, grads, k_out, q_out, latents_out):
    latents_out[...] = latents[...]
    joined = lax.dot_general(
        latents[...], weight[...], (((1,), (0,)), ((), ())), preferred_element_type=F32
    )
    joined_t = joined.T.astype(BF)
    k_out[:NOPE_DIM] = joined_t[:NOPE_DIM]
    k_out[NOPE_DIM:HEAD_DIM] = rot_key[...]
    k_out[HEAD_DIM:] = joined_t[NOPE_DIM:]
    q_t = queries[...].astype(F32)
    g_t = grads[...].astype(F32)
    delta = jnp.sum(outputs[...].astype(F32) * g_t, axis=0, keepdims=True)
    rows = three_parts(logs[...] * (-1.0 / SCALE)) + three_parts(-delta)
    index = lax.broadcasted_iota(jnp.int32, (PAD, TOK), 0)
    pad = jnp.zeros((PAD, TOK), F32)
    for i, row in enumerate(rows):
        pad = jnp.where(index == i, row, pad)
    block = jnp.concatenate([q_t, pad, g_t], axis=0).astype(BF)
    for i in range(GROUP):
        q_out[i] = block


def attend(q_all, k_all, far_out, dkv_out, q_t, q_tok, g_tok, k_t, k_tok, v_tok, dq_acc, dk_acc, dv_acc, dscores, probs_b, far_block, sem):
    total = GROUP * TOK
    lane = lax.broadcasted_iota(jnp.int32, (TOK, PAD), 1)
    key_pad = jnp.where(lane < 3, 1.0, 0.0).astype(F32)
    value_pad = jnp.where((lane >= 3) & (lane < 6), 1.0, 0.0).astype(F32)
    for i in range(GROUP):
        at = slice(i * TOK, (i + 1) * TOK)
        q_block = q_all[i]
        q_t[:, at] = q_block
        tok = q_block.astype(F32).T
        q_tok[at, :] = tok[:, :HEAD_DIM].astype(BF)
        g_tok[at, :] = tok[:, HEAD_DIM + PAD :].astype(BF)
        k_block = k_all[i]
        k_t[:, at] = k_block[:HEAD_DIM]
        ktok = k_block.astype(F32).T
        k_tok[at, :] = jnp.concatenate([ktok[:, :HEAD_DIM], key_pad], axis=1).astype(BF)
        v_tok[at, :] = jnp.concatenate([value_pad, ktok[:, HEAD_DIM:]], axis=1).astype(BF)
    step = 256
    for ki in range(total // step):
        ks = slice(ki * step, (ki + 1) * step)
        for qi in range(total // step):
            qs = slice(qi * step, (qi + 1) * step)
            scores = jnp.dot(k_tok[ks, :], q_t[: HEAD_DIM + PAD, qs], preferred_element_type=F32)
            probs = jnp.exp2(scores * (SCALE * math.log2(math.e)))
            dprob = jnp.dot(v_tok[ks, :], q_t[HEAD_DIM:, qs], preferred_element_type=F32)
            dscores[ks, qs] = (probs * dprob).astype(BF)
            probs_b[ks, qs] = probs.astype(BF)
        dk_acc[ks, :] = jnp.dot(dscores[ks, :], q_tok[...], preferred_element_type=F32)
        dv_acc[ks, :] = jnp.dot(probs_b[ks, :], g_tok[...], preferred_element_type=F32)
    for qi in range(total // step):
        qs = slice(qi * step, (qi + 1) * step)
        dq_acc[:, qs] = jnp.dot(k_t[...], dscores[:, qs], preferred_element_type=F32)
    for i in range(GROUP):
        far_block[i, :HEAD_DIM] = (dq_acc[:, i * TOK : (i + 1) * TOK] * SCALE).astype(BF)
        far_block[i, HEAD_DIM:] = jnp.zeros((8, TOK), BF)
    copy = pltpu.make_async_copy(far_block, far_out, sem)
    copy.start()
    for i in range(GROUP):
        at = slice(i * TOK, (i + 1) * TOK)
        dkv_out[i] = jnp.concatenate(
            [(dk_acc[at, :] * SCALE).T, dv_acc[at, :].T], axis=0
        ).astype(BF)
    copy.wait()


def finish_keys(dkv, latents, key_grad, value_grad, rot_out, weight_out):
    total = dkv[0].astype(F32)
    for i in range(1, GROUP):
        total = total + dkv[i].astype(F32)
    rot_out[...] = total[NOPE_DIM:HEAD_DIM]
    key_grad[...] = total[:NOPE_DIM].astype(BF)
    value_grad[...] = total[HEAD_DIM:].astype(BF)
    stacked = jnp.concatenate([total[:NOPE_DIM], total[HEAD_DIM:]], axis=0).T.astype(BF)
    weight = lax.dot_general(
        latents[...], stacked, (((0,), (0,)), ((), ())), preferred_element_type=F32
    )
    by_owner = weight.reshape(GROUP, GROUP, 8, TOK)
    for i in range(GROUP):
        weight_out[i] = by_owner[:, i].reshape(GROUP * 8, TOK).astype(BF)


def join_far(weight, far_in, far_out, rows, sem):
    del far_in
    total = weight[0].astype(F32)
    for i in range(1, GROUP):
        total = total + weight[i].astype(F32)
    rows[...] = total.reshape(GROUP, 8, TOK).astype(BF)
    copy = pltpu.make_async_copy(rows, far_out.at[:, HEAD_DIM:], sem)
    copy.start()
    copy.wait()


def finish_rest(far, rot, query_grad, weight_grad, rot_grad):
    total = far[0].astype(F32)
    around = rot[0]
    for i in range(1, GROUP):
        total = total + far[i].astype(F32)
        around = around + rot[i]
    query_grad[...] = total[:HEAD_DIM].astype(BF)
    weight_grad[...] = total[HEAD_DIM:]
    rot_grad[...] = around


def call(body, args, outs, name, scratch=(), **more):
    shapes = [
        pltpu.VMEM(shape, kind) if near else jax.ShapeDtypeStruct(shape, kind)
        for shape, kind, near in outs
    ]
    return pl.pallas_call(body, out_shape=shapes, scratch_shapes=list(scratch), name=name, **more)(
        *args
    )


def close(x):
    return pltpu.with_memory_space_constraint(x, pltpu.VMEM)


def exchange(x, axes):
    return close(lax.all_to_all(x, axes, split_axis=0, concat_axis=0, tiled=True))


def gather_pairs(x, axes):
    for axis in axes:
        x = lax.all_gather(x, axis, axis=0)
    return x


def per_device(queries, latents, rot_key, kv_weight, log_sums, outputs, out_grad):
    total = GROUP * TOK
    k_send, q_send, latents_kept = call(
        prepare,
        (latents, rot_key.T, kv_weight, queries.T, log_sums.T, outputs.T, out_grad.T),
        [((K_ROWS, TOK), BF, True), ((GROUP, Q_ROWS, TOK), BF, False), (latents.shape, BF, True)],
        "prepare",
    )
    q_all = exchange(q_send, FAR)
    k_all = close(gather_pairs(k_send, NEAR[::-1]).reshape(GROUP, K_ROWS, TOK))
    far_send, dkv = call(
        attend,
        (q_all, k_all),
        [((GROUP, FAR_ROWS, TOK), BF, False), ((GROUP, K_ROWS, TOK), BF, True)],
        "attend",
        [
            pltpu.VMEM((Q_ROWS, total), BF),
            pltpu.VMEM((total, HEAD_DIM), BF),
            pltpu.VMEM((total, VALUE_DIM), BF),
            pltpu.VMEM((HEAD_DIM, total), BF),
            pltpu.VMEM((total, HEAD_DIM + PAD), BF),
            pltpu.VMEM((total, PAD + VALUE_DIM), BF),
            pltpu.VMEM((HEAD_DIM, total), F32),
            pltpu.VMEM((total, HEAD_DIM), F32),
            pltpu.VMEM((total, VALUE_DIM), F32),
            pltpu.VMEM((total, total), BF),
            pltpu.VMEM((total, total), BF),
            pltpu.VMEM((GROUP, FAR_ROWS, TOK), BF),
            pltpu.SemaphoreType.DMA,
        ],
        out_specs=[pl.BlockSpec(memory_space=pl.ANY), pl.BlockSpec(memory_space=pltpu.VMEM)],
    )
    key_grad, value_grad, rot_send, weight_send = call(
        finish_keys,
        (exchange(dkv, NEAR), close(latents_kept)),
        [
            ((NOPE_DIM, TOK), BF, False),
            ((VALUE_DIM, TOK), BF, False),
            ((ROPE_DIM, TOK), F32, True),
            ((GROUP, GROUP * 8, TOK), BF, True),
        ],
        "finish_keys",
    )
    rot_all = close(gather_pairs(rot_send, HEADS_AXIS[::-1]).reshape(GROUP, ROPE_DIM, TOK))
    (far_send,) = call(
        join_far,
        (exchange(weight_send, NEAR), far_send),
        [((GROUP, FAR_ROWS, TOK), BF, False)],
        "join_far",
        [pltpu.VMEM((GROUP, 8, TOK), BF), pltpu.SemaphoreType.DMA],
        in_specs=[pl.BlockSpec(memory_space=pltpu.VMEM), pl.BlockSpec(memory_space=pl.ANY)],
        out_specs=[pl.BlockSpec(memory_space=pl.ANY)],
        input_output_aliases={1: 0},
    )
    query_grad, weight_grad, rot_grad = call(
        finish_rest,
        (exchange(far_send, FAR), rot_all),
        [((HEAD_DIM, TOK), BF, False), ((8, TOK), F32, False), ((ROPE_DIM, TOK), F32, False)],
        "finish_rest",
    )
    return query_grad.T, key_grad.T, value_grad.T, rot_grad.T, weight_grad


def solution(mesh):
    sp, tp = FAR + NEAR, HEADS_AXIS
    split = Mesh(mesh.devices.reshape((2,) * 9), sp + tp)
    placed = (P(sp, tp), P(sp, None), P(sp, None), P(None, tp), P(sp, tp), P(sp, tp), P(sp, tp))
    return jax.shard_map(
        per_device,
        mesh=split,
        in_specs=placed,
        out_specs=(P(sp, tp), P(sp, tp), P(sp, tp), P(sp, None), P(sp, tp)),
        check_vma=False,
    )
```

```python
import math

import jax
import jax.numpy as jnp
from jax import lax
from jax.experimental import pallas as pl
from jax.experimental.pallas import tpu as pltpu
from jax.sharding import Mesh, PartitionSpec as P

NOPE_DIM = 64
ROPE_DIM = 32
VALUE_DIM = 64
HEAD_DIM = NOPE_DIM + ROPE_DIM
SCALE = HEAD_DIM**-0.5
PAD = 8
FAR_ROWS = HEAD_DIM + 8
Q_ROWS = HEAD_DIM + PAD + VALUE_DIM
K_ROWS = HEAD_DIM + VALUE_DIM
BF = jnp.bfloat16
F32 = jnp.float32

FAR = ("z1", "z2", "z3")
NEAR = ("y0", "y1", "z0")
HEADS_AXIS = ("x1", "x0", "c")
GROUP = 8
TOK = 128


def reverse(index):
    return (index & 1) * 4 + (index & 2) + index // 4


def three_parts(row):
    high = row.astype(BF)
    rest = row - high.astype(F32)
    middle = rest.astype(BF)
    low = (rest - middle.astype(F32)).astype(BF)
    return high.astype(F32), middle.astype(F32), low.astype(F32)


def prepare(latents, rot_key, weight, queries, logs, outputs, grads, k_out, q_out, latents_out):
    latents_out[...] = latents[...]
    joined = lax.dot_general(
        latents[...], weight[...], (((1,), (0,)), ((), ())), preferred_element_type=F32
    )
    joined_t = joined.T.astype(BF)
    k_out[:NOPE_DIM] = joined_t[:NOPE_DIM]
    k_out[NOPE_DIM:HEAD_DIM] = rot_key[...]
    k_out[HEAD_DIM:] = joined_t[NOPE_DIM:]
    q_t = queries[...].astype(F32)
    g_t = grads[...].astype(F32)
    delta = jnp.sum(outputs[...].astype(F32) * g_t, axis=0, keepdims=True)
    rows = three_parts(logs[...] * (-1.0 / SCALE)) + three_parts(-delta)
    index = lax.broadcasted_iota(jnp.int32, (PAD, TOK), 0)
    pad = jnp.zeros((PAD, TOK), F32)
    for i, row in enumerate(rows):
        pad = jnp.where(index == i, row, pad)
    block = jnp.concatenate([q_t, pad, g_t], axis=0).astype(BF)
    for i in range(GROUP):
        q_out[i] = block


def attend(q_all, k_all, dq_out, dkv_out, q_t, q_tok, g_tok, k_t, k_tok, v_tok, dq_acc, dk_acc, dv_acc, dscores, probs_b):
    total = GROUP * TOK
    lane = lax.broadcasted_iota(jnp.int32, (TOK, PAD), 1)
    key_pad = jnp.where(lane < 3, 1.0, 0.0).astype(F32)
    value_pad = jnp.where((lane >= 3) & (lane < 6), 1.0, 0.0).astype(F32)
    for i in range(GROUP):
        at = slice(i * TOK, (i + 1) * TOK)
        q_block = q_all[i]
        q_t[:, at] = q_block
        tok = q_block.astype(F32).T
        q_tok[at, :] = tok[:, :HEAD_DIM].astype(BF)
        g_tok[at, :] = tok[:, HEAD_DIM + PAD :].astype(BF)
        k_block = k_all[reverse(i)]
        k_t[:, at] = k_block[:HEAD_DIM]
        ktok = k_block.astype(F32).T
        k_tok[at, :] = jnp.concatenate([ktok[:, :HEAD_DIM], key_pad], axis=1).astype(BF)
        v_tok[at, :] = jnp.concatenate([value_pad, ktok[:, HEAD_DIM:]], axis=1).astype(BF)
    step = 256
    for ki in range(total // step):
        ks = slice(ki * step, (ki + 1) * step)
        for qi in range(total // step):
            qs = slice(qi * step, (qi + 1) * step)
            scores = jnp.dot(k_tok[ks, :], q_t[: HEAD_DIM + PAD, qs], preferred_element_type=F32)
            probs = jnp.exp2(scores * (SCALE * math.log2(math.e)))
            dprob = jnp.dot(v_tok[ks, :], q_t[HEAD_DIM:, qs], preferred_element_type=F32)
            dscores[ks, qs] = (probs * dprob).astype(BF)
            probs_b[ks, qs] = probs.astype(BF)
        dk_acc[ks, :] = jnp.dot(dscores[ks, :], q_tok[...], preferred_element_type=F32)
        dv_acc[ks, :] = jnp.dot(probs_b[ks, :], g_tok[...], preferred_element_type=F32)
    for qi in range(total // step):
        qs = slice(qi * step, (qi + 1) * step)
        dq_acc[:, qs] = jnp.dot(k_t[...], dscores[:, qs], preferred_element_type=F32)
    for i in range(GROUP):
        at = slice(i * TOK, (i + 1) * TOK)
        dq_out[i] = (dq_acc[:, at] * SCALE).astype(BF)
        dkv_out[i] = jnp.concatenate(
            [(dk_acc[at, :] * SCALE).T, dv_acc[at, :].T], axis=0
        ).astype(BF)


def finish_keys(dkv, latents, key_grad, value_grad, rot_out, weight_out):
    total = dkv[0].astype(F32)
    for i in range(1, GROUP):
        total = total + dkv[i].astype(F32)
    rot_out[...] = total[NOPE_DIM:HEAD_DIM]
    key_grad[...] = total[:NOPE_DIM].astype(BF)
    value_grad[...] = total[HEAD_DIM:].astype(BF)
    stacked = jnp.concatenate([total[:NOPE_DIM], total[HEAD_DIM:]], axis=0).T.astype(BF)
    weight = lax.dot_general(
        latents[...], stacked, (((0,), (0,)), ((), ())), preferred_element_type=F32
    )
    by_owner = weight.reshape(GROUP, GROUP, 8, TOK)
    for i in range(GROUP):
        rows = [by_owner[reverse(k), reverse(i)] for k in range(GROUP)]
        weight_out[i] = jnp.concatenate(rows, axis=0).astype(BF)


def join_far(weight, dq, far_out):
    total = weight[0].astype(F32)
    for i in range(1, GROUP):
        total = total + weight[i].astype(F32)
    for i in range(GROUP):
        far_out[i, :HEAD_DIM] = dq[i]
        far_out[i, HEAD_DIM:] = total[i * 8 : (i + 1) * 8].astype(BF)


def finish_rest(far, rot, query_grad, weight_grad, rot_grad):
    total = far[0].astype(F32)
    around = rot[0]
    for i in range(1, GROUP):
        total = total + far[i].astype(F32)
        around = around + rot[i]
    query_grad[...] = total[:HEAD_DIM].astype(BF)
    weight_grad[...] = total[HEAD_DIM:]
    rot_grad[...] = around


def call(body, args, outs, name, scratch=()):
    shapes = [
        pltpu.VMEM(shape, kind) if near else jax.ShapeDtypeStruct(shape, kind)
        for shape, kind, near in outs
    ]
    return pl.pallas_call(body, out_shape=shapes, scratch_shapes=list(scratch), name=name)(*args)


def close(x):
    return pltpu.with_memory_space_constraint(x, pltpu.VMEM)


def exchange(x, axes):
    return close(lax.all_to_all(x, axes, split_axis=0, concat_axis=0, tiled=True))


def gather_pairs(x, axes):
    for axis in axes:
        x = lax.all_gather(x, axis, axis=0)
    return x


def per_device(queries, latents, rot_key, kv_weight, log_sums, outputs, out_grad):
    total = GROUP * TOK
    k_send, q_send, latents_kept = call(
        prepare,
        (latents, rot_key.T, kv_weight, queries.T, log_sums.T, outputs.T, out_grad.T),
        [((K_ROWS, TOK), BF, True), ((GROUP, Q_ROWS, TOK), BF, False), (latents.shape, BF, True)],
        "prepare",
    )
    q_all = exchange(q_send, FAR)
    k_all = close(gather_pairs(k_send, NEAR).reshape(GROUP, K_ROWS, TOK))
    dq, dkv = call(
        attend,
        (q_all, k_all),
        [((GROUP, HEAD_DIM, TOK), BF, True), ((GROUP, K_ROWS, TOK), BF, True)],
        "attend",
        [
            pltpu.VMEM((Q_ROWS, total), BF),
            pltpu.VMEM((total, HEAD_DIM), BF),
            pltpu.VMEM((total, VALUE_DIM), BF),
            pltpu.VMEM((HEAD_DIM, total), BF),
            pltpu.VMEM((total, HEAD_DIM + PAD), BF),
            pltpu.VMEM((total, PAD + VALUE_DIM), BF),
            pltpu.VMEM((HEAD_DIM, total), F32),
            pltpu.VMEM((total, HEAD_DIM), F32),
            pltpu.VMEM((total, VALUE_DIM), F32),
            pltpu.VMEM((total, total), BF),
            pltpu.VMEM((total, total), BF),
        ],
    )
    key_grad, value_grad, rot_send, weight_send = call(
        finish_keys,
        (exchange(dkv, NEAR), close(latents_kept)),
        [
            ((NOPE_DIM, TOK), BF, False),
            ((VALUE_DIM, TOK), BF, False),
            ((ROPE_DIM, TOK), F32, True),
            ((GROUP, GROUP * 8, TOK), BF, True),
        ],
        "finish_keys",
    )
    rot_all = close(gather_pairs(rot_send, HEADS_AXIS[::-1]).reshape(GROUP, ROPE_DIM, TOK))
    (far_send,) = call(
        join_far,
        (exchange(weight_send, NEAR), close(dq)),
        [((GROUP, FAR_ROWS, TOK), BF, False)],
        "join_far",
    )
    query_grad, weight_grad, rot_grad = call(
        finish_rest,
        (exchange(far_send, FAR), rot_all),
        [((HEAD_DIM, TOK), BF, False), ((8, TOK), F32, False), ((ROPE_DIM, TOK), F32, False)],
        "finish_rest",
    )
    return query_grad.T, key_grad.T, value_grad.T, rot_grad.T, weight_grad


def solution(mesh):
    sp, tp = FAR[::-1] + NEAR[::-1], HEADS_AXIS
    split = Mesh(mesh.devices.reshape((2,) * 9), sp + tp)
    placed = (P(sp, tp), P(sp, None), P(sp, None), P(None, tp), P(sp, tp), P(sp, tp), P(sp, tp))
    return jax.shard_map(
        per_device,
        mesh=split,
        in_specs=placed,
        out_specs=(P(sp, tp), P(sp, tp), P(sp, tp), P(sp, None), P(sp, tp)),
        check_vma=False,
    )
```

```python
import math

import jax
import jax.numpy as jnp
from jax import lax
from jax.experimental import pallas as pl
from jax.experimental.pallas import tpu as pltpu
from jax.sharding import Mesh, PartitionSpec as P


NOPE_DIM = 64
ROPE_DIM = 32
VALUE_DIM = 64
HEAD_DIM = NOPE_DIM + ROPE_DIM
SCALE = HEAD_DIM**-0.5
PAD = 8
FAR_ROWS = HEAD_DIM + 8
Q_ROWS = HEAD_DIM + PAD + VALUE_DIM
K_ROWS = HEAD_DIM + VALUE_DIM
BF = jnp.bfloat16
F32 = jnp.float32

FAR = ("z1", "z2", "z3")
NEAR = ("y0", "y1", "z0")
HEADS_AXIS = ("x1", "x0", "c")
GROUP = 8
TOK = 128


def reverse(index):
    return (index & 1) * 4 + (index & 2) + index // 4


def three_parts(row):
    high = row.astype(BF)
    rest = row - high.astype(F32)
    middle = rest.astype(BF)
    low = (rest - middle.astype(F32)).astype(BF)
    return high.astype(F32), middle.astype(F32), low.astype(F32)


def prepare(latents, rot_key, weight, queries, logs, outputs, grads, k_out, q_out, latents_out):
    latents_out[...] = latents[...]
    joined = lax.dot_general(
        latents[...], weight[...], (((1,), (0,)), ((), ())), preferred_element_type=F32
    )
    joined_t = joined.T.astype(BF)
    k_out[:NOPE_DIM] = joined_t[:NOPE_DIM]
    k_out[NOPE_DIM:HEAD_DIM] = rot_key[...]
    k_out[HEAD_DIM:] = joined_t[NOPE_DIM:]
    q_t = queries[...].astype(F32)
    g_t = grads[...].astype(F32)
    delta = jnp.sum(outputs[...].astype(F32) * g_t, axis=0, keepdims=True)
    rows = three_parts(logs[...] * (-1.0 / SCALE)) + three_parts(-delta)
    index = lax.broadcasted_iota(jnp.int32, (PAD, TOK), 0)
    pad = jnp.zeros((PAD, TOK), F32)
    for i, row in enumerate(rows):
        pad = jnp.where(index == i, row, pad)
    block = jnp.concatenate([q_t, pad, g_t], axis=0).astype(BF)
    for i in range(GROUP):
        q_out[i] = block


def pair(own, other, out):
    out[0] = own[...]
    out[1] = other[...]


def attend(side, q_all, k_all, dq_out, dkv_out, q_t, q_tok, g_tok, k_t, k_tok, v_tok, dq_acc, dk_acc, dv_acc, dscores, probs_b):
    total = GROUP * TOK
    lane = lax.broadcasted_iota(jnp.int32, (TOK, PAD), 1)
    key_pad = jnp.where(lane < 3, 1.0, 0.0).astype(F32)
    value_pad = jnp.where((lane >= 3) & (lane < 6), 1.0, 0.0).astype(F32)
    for i in range(GROUP):
        at = slice(i * TOK, (i + 1) * TOK)
        q_block = q_all[i]
        q_t[:, at] = q_block
        tok = q_block.astype(F32).T
        q_tok[at, :] = tok[:, :HEAD_DIM].astype(BF)
        g_tok[at, :] = tok[:, HEAD_DIM + PAD :].astype(BF)
        y_index = (i & 2) + i // 4
        k_block = k_all[y_index * 2 + (side[0] ^ (i & 1))]
        k_t[:, at] = k_block[:HEAD_DIM]
        ktok = k_block.astype(F32).T
        k_tok[at, :] = jnp.concatenate([ktok[:, :HEAD_DIM], key_pad], axis=1).astype(BF)
        v_tok[at, :] = jnp.concatenate([value_pad, ktok[:, HEAD_DIM:]], axis=1).astype(BF)
    step = 256
    for ki in range(total // step):
        ks = slice(ki * step, (ki + 1) * step)
        for qi in range(total // step):
            qs = slice(qi * step, (qi + 1) * step)
            scores = jnp.dot(k_tok[ks, :], q_t[: HEAD_DIM + PAD, qs], preferred_element_type=F32)
            probs = jnp.exp2(scores * (SCALE * math.log2(math.e)))
            dprob = jnp.dot(v_tok[ks, :], q_t[HEAD_DIM:, qs], preferred_element_type=F32)
            dscores[ks, qs] = (probs * dprob).astype(BF)
            probs_b[ks, qs] = probs.astype(BF)
        dk_acc[ks, :] = jnp.dot(dscores[ks, :], q_tok[...], preferred_element_type=F32)
        dv_acc[ks, :] = jnp.dot(probs_b[ks, :], g_tok[...], preferred_element_type=F32)
    for qi in range(total // step):
        qs = slice(qi * step, (qi + 1) * step)
        dq_acc[:, qs] = jnp.dot(k_t[...], dscores[:, qs], preferred_element_type=F32)
    for i in range(GROUP):
        at = slice(i * TOK, (i + 1) * TOK)
        dq_out[i] = (dq_acc[:, at] * SCALE).astype(BF)
        dkv_out[i] = jnp.concatenate(
            [(dk_acc[at, :] * SCALE).T, dv_acc[at, :].T], axis=0
        ).astype(BF)


def finish_keys(dkv, latents, key_grad, value_grad, rot_out, weight_out):
    total = dkv[0].astype(F32)
    for i in range(1, GROUP):
        total = total + dkv[i].astype(F32)
    rot_out[...] = total[NOPE_DIM:HEAD_DIM]
    key_grad[...] = total[:NOPE_DIM].astype(BF)
    value_grad[...] = total[HEAD_DIM:].astype(BF)
    stacked = jnp.concatenate([total[:NOPE_DIM], total[HEAD_DIM:]], axis=0).T.astype(BF)
    weight = lax.dot_general(
        latents[...], stacked, (((0,), (0,)), ((), ())), preferred_element_type=F32
    )
    by_owner = weight.reshape(GROUP, GROUP, 8, TOK)
    for i in range(GROUP):
        rows = [by_owner[reverse(k), reverse(i)] for k in range(GROUP)]
        weight_out[i] = jnp.concatenate(rows, axis=0).astype(BF)


def join_far(weight, dq, far_out):
    total = weight[0].astype(F32)
    for i in range(1, GROUP):
        total = total + weight[i].astype(F32)
    for i in range(GROUP):
        far_out[i, :HEAD_DIM] = dq[i]
        far_out[i, HEAD_DIM:] = total[i * 8 : (i + 1) * 8].astype(BF)


def finish_rest(far, rot, query_grad, weight_grad, rot_grad):
    total = far[0].astype(F32)
    around = rot[0]
    for i in range(1, GROUP):
        total = total + far[i].astype(F32)
        around = around + rot[i]
    query_grad[...] = total[:HEAD_DIM].astype(BF)
    weight_grad[...] = total[HEAD_DIM:]
    rot_grad[...] = around


def call(body, args, outs, scratch=(), **more):
    shapes = [
        pltpu.VMEM(shape, kind) if near else jax.ShapeDtypeStruct(shape, kind)
        for shape, kind, near in outs
    ]
    return pl.pallas_call(body, out_shape=shapes, scratch_shapes=list(scratch), **more)(*args)


def close(x):
    return pltpu.with_memory_space_constraint(x, pltpu.VMEM)


def exchange(x, axes):
    return close(lax.all_to_all(x, axes, split_axis=0, concat_axis=0, tiled=True))


def gather_pairs(x, axes):
    for axis in axes:
        x = lax.all_gather(x, axis, axis=0)
    return x


def per_device(queries, latents, rot_key, kv_weight, log_sums, outputs, out_grad):
    total = GROUP * TOK
    k_send, q_send, latents_kept = call(
        prepare,
        (latents, rot_key.T, kv_weight, queries.T, log_sums.T, outputs.T, out_grad.T),
        [((K_ROWS, TOK), BF, True), ((GROUP, Q_ROWS, TOK), BF, False), (latents.shape, BF, True)],
    )
    k_other = lax.ppermute(k_send, "z0", ((0, 1), (1, 0)))
    q_all = exchange(q_send, FAR)
    (k_pair,) = call(pair, (close(k_send), close(k_other)), [((2, K_ROWS, TOK), BF, True)])
    k_all = close(gather_pairs(k_pair, NEAR[:2]).reshape(GROUP, K_ROWS, TOK))
    side = lax.axis_index("z0").astype(jnp.int32).reshape(1)
    dq, dkv = call(
        attend,
        (side, q_all, k_all),
        [((GROUP, HEAD_DIM, TOK), BF, True), ((GROUP, K_ROWS, TOK), BF, True)],
        [
            pltpu.VMEM((Q_ROWS, total), BF),
            pltpu.VMEM((total, HEAD_DIM), BF),
            pltpu.VMEM((total, VALUE_DIM), BF),
            pltpu.VMEM((HEAD_DIM, total), BF),
            pltpu.VMEM((total, HEAD_DIM + PAD), BF),
            pltpu.VMEM((total, PAD + VALUE_DIM), BF),
            pltpu.VMEM((HEAD_DIM, total), F32),
            pltpu.VMEM((total, HEAD_DIM), F32),
            pltpu.VMEM((total, VALUE_DIM), F32),
            pltpu.VMEM((total, total), BF),
            pltpu.VMEM((total, total), BF),
        ],
        in_specs=[pl.BlockSpec(memory_space=where) for where in (pltpu.SMEM, pltpu.VMEM, pltpu.VMEM)],
    )
    key_grad, value_grad, rot_send, weight_send = call(
        finish_keys,
        (exchange(dkv, NEAR), close(latents_kept)),
        [
            ((NOPE_DIM, TOK), BF, False),
            ((VALUE_DIM, TOK), BF, False),
            ((ROPE_DIM, TOK), F32, True),
            ((GROUP, GROUP * 8, TOK), BF, True),
        ],
    )
    rot_all = close(gather_pairs(rot_send, HEADS_AXIS[::-1]).reshape(GROUP, ROPE_DIM, TOK))
    (far_send,) = call(
        join_far, (exchange(weight_send, NEAR), close(dq)), [((GROUP, FAR_ROWS, TOK), BF, False)]
    )
    query_grad, weight_grad, rot_grad = call(
        finish_rest,
        (exchange(far_send, FAR), rot_all),
        [((HEAD_DIM, TOK), BF, False), ((8, TOK), F32, False), ((ROPE_DIM, TOK), F32, False)],
    )
    return query_grad.T, key_grad.T, value_grad.T, rot_grad.T, weight_grad


def solution(mesh):
    sp, tp = FAR[::-1] + NEAR[::-1], HEADS_AXIS
    split = Mesh(mesh.devices.reshape((2,) * 9), sp + tp)
    placed = (P(sp, tp), P(sp, None), P(sp, None), P(None, tp), P(sp, tp), P(sp, tp), P(sp, tp))
    return jax.shard_map(
        per_device,
        mesh=split,
        in_specs=placed,
        out_specs=(P(sp, tp), P(sp, tp), P(sp, tp), P(sp, None), P(sp, tp)),
        check_vma=False,
    )
```

```python
import math

import jax
import jax.numpy as jnp
from jax import lax
from jax.experimental import pallas as pl
from jax.experimental.pallas import tpu as pltpu
from jax.sharding import PartitionSpec as P


NOPE_DIM = 64
ROPE_DIM = 32
VALUE_DIM = 64
HEAD_DIM = NOPE_DIM + ROPE_DIM
SCALE = HEAD_DIM**-0.5
PAD = 8
FAR_ROWS = HEAD_DIM + 8
Q_ROWS = HEAD_DIM + PAD + VALUE_DIM
K_ROWS = HEAD_DIM + VALUE_DIM
BF = jnp.bfloat16
F32 = jnp.float32

OUT_ORDER = (8, 0, 12, 4, 10, 2, 14, 6)
BACK_ORDER = (0, 8, 4, 12, 2, 10, 6, 14)
OUT, BACK = (
    [[(z + low) * 4 + y for z in order] for low in range(2) for y in range(4)]
    for order in (OUT_ORDER, BACK_ORDER)
)
NEAR_ORDER = ((0, 0), (1, 0), (0, 2), (1, 2), (0, 1), (1, 1), (0, 3), (1, 3))
NEAR = [[(high + z) * 4 + y for z, y in NEAR_ORDER] for high in range(0, 16, 2)]
GROUP = 8
TOK = 128


def pairs(count, bit):
    return [[i, i + bit] for i in range(count) if not i & bit]


def three_parts(row):
    high = row.astype(BF)
    rest = row - high.astype(F32)
    middle = rest.astype(BF)
    low = (rest - middle.astype(F32)).astype(BF)
    return high.astype(F32), middle.astype(F32), low.astype(F32)


def prepare(latents, rot_key, weight, queries, logs, outputs, grads, k_out, q_out, latents_out):
    latents_out[...] = latents[...]
    joined = lax.dot_general(
        latents[...], weight[...], (((1,), (0,)), ((), ())), preferred_element_type=F32
    )
    joined_t = joined.T.astype(BF)
    k_out[:NOPE_DIM] = joined_t[:NOPE_DIM]
    k_out[NOPE_DIM:HEAD_DIM] = rot_key[...]
    k_out[HEAD_DIM:] = joined_t[NOPE_DIM:]
    q_t = queries[...].astype(F32)
    g_t = grads[...].astype(F32)
    delta = jnp.sum(outputs[...].astype(F32) * g_t, axis=0, keepdims=True)
    rows = three_parts(logs[...] * (-1.0 / SCALE)) + three_parts(-delta)
    index = lax.broadcasted_iota(jnp.int32, (PAD, TOK), 0)
    pad = jnp.zeros((PAD, TOK), F32)
    for i, row in enumerate(rows):
        pad = jnp.where(index == i, row, pad)
    block = jnp.concatenate([q_t, pad, g_t], axis=0).astype(BF)
    for i in range(GROUP):
        q_out[i] = block


def pair(own, other, out):
    out[0] = own[...]
    out[1] = other[...]


def attend(side, q_all, k_all, dq_out, dkv_out, q_t, q_tok, g_tok, k_t, k_tok, v_tok, dq_acc, dk_acc, dv_acc, dscores, probs_b):
    total = GROUP * TOK
    lane = lax.broadcasted_iota(jnp.int32, (TOK, PAD), 1)
    key_pad = jnp.where(lane < 3, 1.0, 0.0).astype(F32)
    value_pad = jnp.where((lane >= 3) & (lane < 6), 1.0, 0.0).astype(F32)
    for i in range(GROUP):
        at = slice(i * TOK, (i + 1) * TOK)
        q_block = q_all[i]
        q_t[:, at] = q_block
        tok = q_block.astype(F32).T
        q_tok[at, :] = tok[:, :HEAD_DIM].astype(BF)
        g_tok[at, :] = tok[:, HEAD_DIM + PAD :].astype(BF)
        low, y = NEAR_ORDER[i]
        k_block = k_all[y * 2 + (side[0] ^ low)]
        k_t[:, at] = k_block[:HEAD_DIM]
        ktok = k_block.astype(F32).T
        k_tok[at, :] = jnp.concatenate([ktok[:, :HEAD_DIM], key_pad], axis=1).astype(BF)
        v_tok[at, :] = jnp.concatenate([value_pad, ktok[:, HEAD_DIM:]], axis=1).astype(BF)
    step = 256
    for ki in range(total // step):
        ks = slice(ki * step, (ki + 1) * step)
        for qi in range(total // step):
            qs = slice(qi * step, (qi + 1) * step)
            scores = jnp.dot(k_tok[ks, :], q_t[: HEAD_DIM + PAD, qs], preferred_element_type=F32)
            probs = jnp.exp2(scores * (SCALE * math.log2(math.e)))
            dprob = jnp.dot(v_tok[ks, :], q_t[HEAD_DIM:, qs], preferred_element_type=F32)
            dscores[ks, qs] = (probs * dprob).astype(BF)
            probs_b[ks, qs] = probs.astype(BF)
        dk_acc[ks, :] = jnp.dot(dscores[ks, :], q_tok[...], preferred_element_type=F32)
        dv_acc[ks, :] = jnp.dot(probs_b[ks, :], g_tok[...], preferred_element_type=F32)
    for qi in range(total // step):
        qs = slice(qi * step, (qi + 1) * step)
        dq_acc[:, qs] = jnp.dot(k_t[...], dscores[:, qs], preferred_element_type=F32)
    for i in range(GROUP):
        at = slice(i * TOK, (i + 1) * TOK)
        dq_out[BACK_ORDER.index(OUT_ORDER[i])] = (dq_acc[:, at] * SCALE).astype(BF)
        dkv_out[i] = jnp.concatenate(
            [(dk_acc[at, :] * SCALE).T, dv_acc[at, :].T], axis=0
        ).astype(BF)


def finish_keys(dkv, latents, key_grad, value_grad, rot_out, weight_out):
    total = dkv[0].astype(F32)
    for i in range(1, GROUP):
        total = total + dkv[i].astype(F32)
    rot_out[...] = total[NOPE_DIM:HEAD_DIM]
    key_grad[...] = total[:NOPE_DIM].astype(BF)
    value_grad[...] = total[HEAD_DIM:].astype(BF)
    stacked = jnp.concatenate([total[:NOPE_DIM], total[HEAD_DIM:]], axis=0).T.astype(BF)
    weight = lax.dot_general(
        latents[...], stacked, (((0,), (0,)), ((), ())), preferred_element_type=F32
    )
    by_owner = weight.reshape(GROUP, GROUP, 8, TOK)
    for i in range(GROUP):
        low, y = NEAR_ORDER[i]
        rows = [by_owner[z // 2, low * 4 + y] for z in BACK_ORDER]
        weight_out[i] = jnp.concatenate(rows, axis=0).astype(BF)


def join_far(weight, dq, far_out):
    total = weight[0].astype(F32)
    for i in range(1, GROUP):
        total = total + weight[i].astype(F32)
    for i in range(GROUP):
        far_out[i, :HEAD_DIM] = dq[i]
        far_out[i, HEAD_DIM:] = total[i * 8 : (i + 1) * 8].astype(BF)


def finish_rest(far, rot, query_grad, weight_grad, rot_grad):
    total = far[0].astype(F32)
    around = rot[0]
    for i in range(1, GROUP):
        total = total + far[i].astype(F32)
        around = around + rot[i]
    query_grad[...] = total[:HEAD_DIM].astype(BF)
    weight_grad[...] = total[HEAD_DIM:]
    rot_grad[...] = around


def call(body, args, outs, scratch=(), **more):
    shapes = [
        pltpu.VMEM(shape, kind) if near else jax.ShapeDtypeStruct(shape, kind)
        for shape, kind, near in outs
    ]
    return pl.pallas_call(body, out_shape=shapes, scratch_shapes=list(scratch), **more)(*args)


def close(x):
    return pltpu.with_memory_space_constraint(x, pltpu.VMEM)


def exchange(x, groups):
    return close(lax.all_to_all(x, "sp", 0, 0, axis_index_groups=groups, tiled=True))


def gather_pairs(x, axis, count, bits):
    for bit in bits:
        x = lax.all_gather(x, axis, axis_index_groups=pairs(count, bit))
    return x


def per_device(queries, latents, rot_key, kv_weight, log_sums, outputs, out_grad):
    total = GROUP * TOK
    k_send, q_send, latents_kept = call(
        prepare,
        (latents, rot_key.T, kv_weight, queries.T, log_sums.T, outputs.T, out_grad.T),
        [((K_ROWS, TOK), BF, True), ((GROUP, Q_ROWS, TOK), BF, False), (latents.shape, BF, True)],
    )
    k_other = lax.ppermute(k_send, "sp", [(i, i ^ 4) for i in range(64)])
    q_all = exchange(q_send, OUT)
    (k_pair,) = call(pair, (close(k_send), close(k_other)), [((2, K_ROWS, TOK), BF, True)])
    k_all = close(gather_pairs(k_pair, "sp", 64, (1, 2)).reshape(GROUP, K_ROWS, TOK))
    side = (lax.axis_index("sp") // 4 % 2).astype(jnp.int32).reshape(1)
    dq, dkv = call(
        attend,
        (side, q_all, k_all),
        [((GROUP, HEAD_DIM, TOK), BF, True), ((GROUP, K_ROWS, TOK), BF, True)],
        [
            pltpu.VMEM((Q_ROWS, total), BF),
            pltpu.VMEM((total, HEAD_DIM), BF),
            pltpu.VMEM((total, VALUE_DIM), BF),
            pltpu.VMEM((HEAD_DIM, total), BF),
            pltpu.VMEM((total, HEAD_DIM + PAD), BF),
            pltpu.VMEM((total, PAD + VALUE_DIM), BF),
            pltpu.VMEM((HEAD_DIM, total), F32),
            pltpu.VMEM((total, HEAD_DIM), F32),
            pltpu.VMEM((total, VALUE_DIM), F32),
            pltpu.VMEM((total, total), BF),
            pltpu.VMEM((total, total), BF),
        ],
        in_specs=[pl.BlockSpec(memory_space=where) for where in (pltpu.SMEM, pltpu.VMEM, pltpu.VMEM)],
    )
    key_grad, value_grad, rot_send, weight_send = call(
        finish_keys,
        (exchange(dkv, NEAR), close(latents_kept)),
        [
            ((NOPE_DIM, TOK), BF, False),
            ((VALUE_DIM, TOK), BF, False),
            ((ROPE_DIM, TOK), F32, True),
            ((GROUP, GROUP * 8, TOK), BF, True),
        ],
    )
    rot_all = close(gather_pairs(rot_send, "tp", 8, (1, 2, 4)).reshape(GROUP, ROPE_DIM, TOK))
    (far_send,) = call(
        join_far, (exchange(weight_send, NEAR), close(dq)), [((GROUP, FAR_ROWS, TOK), BF, False)]
    )
    query_grad, weight_grad, rot_grad = call(
        finish_rest,
        (exchange(far_send, BACK), rot_all),
        [((HEAD_DIM, TOK), BF, False), ((8, TOK), F32, False), ((ROPE_DIM, TOK), F32, False)],
    )
    return query_grad.T, key_grad.T, value_grad.T, rot_grad.T, weight_grad


def solution(mesh):
    placed = (P("sp", "tp"), P("sp", None), P("sp", None), P(None, "tp"), P("sp", "tp"), P("sp", "tp"), P("sp", "tp"))
    return jax.shard_map(
        per_device,
        mesh=mesh,
        in_specs=placed,
        out_specs=(P("sp", "tp"), P("sp", "tp"), P("sp", "tp"), P("sp", None), P("sp", "tp")),
        check_vma=False,
    )
```

```python
import math

import jax
import jax.numpy as jnp
from jax import lax
from jax.experimental import pallas as pl
from jax.experimental.pallas import tpu as pltpu
from jax.sharding import PartitionSpec as P


NOPE_DIM = 64
ROPE_DIM = 32
VALUE_DIM = 64
HEAD_DIM = NOPE_DIM + ROPE_DIM
SCALE = HEAD_DIM**-0.5
PAD = 8
FAR_ROWS = HEAD_DIM + 8
Q_ROWS = HEAD_DIM + PAD + VALUE_DIM
K_ROWS = HEAD_DIM + VALUE_DIM
BF = jnp.bfloat16
F32 = jnp.float32

OUT_ORDER = (8, 0, 12, 4, 10, 2, 14, 6)
BACK_ORDER = (0, 8, 4, 12, 2, 10, 6, 14)
OUT, BACK = (
    [[(z + low) * 4 + y for z in order] for low in range(2) for y in range(4)]
    for order in (OUT_ORDER, BACK_ORDER)
)
NEAR_ORDER = ((0, 0), (1, 0), (0, 2), (1, 2), (0, 1), (1, 1), (0, 3), (1, 3))
NEAR = [[(high + z) * 4 + y for z, y in NEAR_ORDER] for high in range(0, 16, 2)]
GROUP = 8
TOK = 128


def pairs(count, bit):
    return [[i, i + bit] for i in range(count) if not i & bit]


def three_parts(row):
    high = row.astype(BF)
    rest = row - high.astype(F32)
    middle = rest.astype(BF)
    low = (rest - middle.astype(F32)).astype(BF)
    return high.astype(F32), middle.astype(F32), low.astype(F32)


def prepare_keys(latents, rot_key, weight, k_out, latents_out):
    latents_out[...] = latents[...]
    joined = lax.dot_general(
        latents[...], weight[...], (((1,), (0,)), ((), ())), preferred_element_type=F32
    )
    joined_t = joined.T.astype(BF)
    k_out[:NOPE_DIM] = joined_t[:NOPE_DIM]
    k_out[NOPE_DIM:HEAD_DIM] = rot_key[...]
    k_out[HEAD_DIM:] = joined_t[NOPE_DIM:]


def prepare_queries(queries, logs, outputs, grads, q_out):
    q_t = queries[...].astype(F32)
    g_t = grads[...].astype(F32)
    delta = jnp.sum(outputs[...].astype(F32) * g_t, axis=0, keepdims=True)
    rows = three_parts(logs[...] * (-1.0 / SCALE)) + three_parts(-delta)
    index = lax.broadcasted_iota(jnp.int32, (PAD, TOK), 0)
    pad = jnp.zeros((PAD, TOK), F32)
    for i, row in enumerate(rows):
        pad = jnp.where(index == i, row, pad)
    block = jnp.concatenate([q_t, pad, g_t], axis=0).astype(BF)
    for i in range(GROUP):
        q_out[i] = block


def attend(q_all, k_all, dq_out, dkv_out, q_t, q_tok, g_tok, k_t, k_tok, v_tok, dq_acc, dk_acc, dv_acc, dscores, probs_b):
    total = GROUP * TOK
    lane = lax.broadcasted_iota(jnp.int32, (TOK, PAD), 1)
    key_pad = jnp.where(lane < 3, 1.0, 0.0).astype(F32)
    value_pad = jnp.where((lane >= 3) & (lane < 6), 1.0, 0.0).astype(F32)
    for i in range(GROUP):
        at = slice(i * TOK, (i + 1) * TOK)
        q_block = q_all[i]
        q_t[:, at] = q_block
        tok = q_block.astype(F32).T
        q_tok[at, :] = tok[:, :HEAD_DIM].astype(BF)
        g_tok[at, :] = tok[:, HEAD_DIM + PAD :].astype(BF)
        low, y = NEAR_ORDER[i]
        k_block = k_all[low * 4 + y]
        k_t[:, at] = k_block[:HEAD_DIM]
        ktok = k_block.astype(F32).T
        k_tok[at, :] = jnp.concatenate([ktok[:, :HEAD_DIM], key_pad], axis=1).astype(BF)
        v_tok[at, :] = jnp.concatenate([value_pad, ktok[:, HEAD_DIM:]], axis=1).astype(BF)
    step = 256
    for ki in range(total // step):
        ks = slice(ki * step, (ki + 1) * step)
        for qi in range(total // step):
            qs = slice(qi * step, (qi + 1) * step)
            scores = jnp.dot(k_tok[ks, :], q_t[: HEAD_DIM + PAD, qs], preferred_element_type=F32)
            probs = jnp.exp2(scores * (SCALE * math.log2(math.e)))
            dprob = jnp.dot(v_tok[ks, :], q_t[HEAD_DIM:, qs], preferred_element_type=F32)
            dscores[ks, qs] = (probs * dprob).astype(BF)
            probs_b[ks, qs] = probs.astype(BF)
        dk_acc[ks, :] = jnp.dot(dscores[ks, :], q_tok[...], preferred_element_type=F32)
        dv_acc[ks, :] = jnp.dot(probs_b[ks, :], g_tok[...], preferred_element_type=F32)
    for qi in range(total // step):
        qs = slice(qi * step, (qi + 1) * step)
        dq_acc[:, qs] = jnp.dot(k_t[...], dscores[:, qs], preferred_element_type=F32)
    for i in range(GROUP):
        at = slice(i * TOK, (i + 1) * TOK)
        dq_out[BACK_ORDER.index(OUT_ORDER[i])] = (dq_acc[:, at] * SCALE).astype(BF)
        dkv_out[i] = jnp.concatenate(
            [(dk_acc[at, :] * SCALE).T, dv_acc[at, :].T], axis=0
        ).astype(BF)


def finish_keys(dkv, latents, key_grad, value_grad, rot_out, weight_out):
    total = dkv[0].astype(F32)
    for i in range(1, GROUP):
        total = total + dkv[i].astype(F32)
    rot_out[...] = total[NOPE_DIM:HEAD_DIM]
    key_grad[...] = total[:NOPE_DIM].astype(BF)
    value_grad[...] = total[HEAD_DIM:].astype(BF)
    stacked = jnp.concatenate([total[:NOPE_DIM], total[HEAD_DIM:]], axis=0).T.astype(BF)
    weight = lax.dot_general(
        latents[...], stacked, (((0,), (0,)), ((), ())), preferred_element_type=F32
    )
    by_owner = weight.reshape(GROUP, GROUP, 8, TOK)
    for i in range(GROUP):
        low, y = NEAR_ORDER[i]
        rows = [by_owner[z // 2, low * 4 + y] for z in BACK_ORDER]
        weight_out[i] = jnp.concatenate(rows, axis=0).astype(BF)


def join_far(weight, dq, far_out):
    total = weight[0].astype(F32)
    for i in range(1, GROUP):
        total = total + weight[i].astype(F32)
    for i in range(GROUP):
        far_out[i, :HEAD_DIM] = dq[i]
        far_out[i, HEAD_DIM:] = total[i * 8 : (i + 1) * 8].astype(BF)


def finish_rest(far, rot, query_grad, weight_grad, rot_grad):
    total = far[0].astype(F32)
    around = rot[0]
    for i in range(1, GROUP):
        total = total + far[i].astype(F32)
        around = around + rot[i]
    query_grad[...] = total[:HEAD_DIM].astype(BF)
    weight_grad[...] = total[HEAD_DIM:]
    rot_grad[...] = around


def call(body, args, outs, name, scratch=(), **more):
    shapes = [
        pltpu.VMEM(shape, kind) if near else jax.ShapeDtypeStruct(shape, kind)
        for shape, kind, near in outs
    ]
    return pl.pallas_call(body, out_shape=shapes, scratch_shapes=list(scratch), name=name, **more)(
        *args
    )


def close(x):
    return pltpu.with_memory_space_constraint(x, pltpu.VMEM)


def exchange(x, groups):
    return close(lax.all_to_all(x, "sp", 0, 0, axis_index_groups=groups, tiled=True))


def gather_pairs(x, axis, count, bits):
    for bit in bits:
        x = lax.all_gather(x, axis, axis_index_groups=pairs(count, bit))
    return x


def per_device(queries, latents, rot_key, kv_weight, log_sums, outputs, out_grad):
    total = GROUP * TOK
    (q_send,) = call(
        prepare_queries,
        (queries.T, log_sums.T, outputs.T, out_grad.T),
        [((GROUP, Q_ROWS, TOK), BF, False)],
        "prepare_queries",
    )
    k_send, latents_kept = call(
        prepare_keys,
        (latents, rot_key.T, kv_weight),
        [((K_ROWS, TOK), BF, True), (latents.shape, BF, True)],
        "prepare_keys",
    )
    q_all = exchange(q_send, OUT)
    k_all = close(gather_pairs(k_send, "sp", 64, (1, 2, 4)).reshape(GROUP, K_ROWS, TOK))
    dq, dkv = call(
        attend,
        (q_all, k_all),
        [((GROUP, HEAD_DIM, TOK), BF, True), ((GROUP, K_ROWS, TOK), BF, True)],
        "attend",
        [
            pltpu.VMEM((Q_ROWS, total), BF),
            pltpu.VMEM((total, HEAD_DIM), BF),
            pltpu.VMEM((total, VALUE_DIM), BF),
            pltpu.VMEM((HEAD_DIM, total), BF),
            pltpu.VMEM((total, HEAD_DIM + PAD), BF),
            pltpu.VMEM((total, PAD + VALUE_DIM), BF),
            pltpu.VMEM((HEAD_DIM, total), F32),
            pltpu.VMEM((total, HEAD_DIM), F32),
            pltpu.VMEM((total, VALUE_DIM), F32),
            pltpu.VMEM((total, total), BF),
            pltpu.VMEM((total, total), BF),
        ],
    )
    key_grad, value_grad, rot_send, weight_send = call(
        finish_keys,
        (exchange(dkv, NEAR), close(latents_kept)),
        [
            ((NOPE_DIM, TOK), BF, False),
            ((VALUE_DIM, TOK), BF, False),
            ((ROPE_DIM, TOK), F32, True),
            ((GROUP, GROUP * 8, TOK), BF, True),
        ],
        "finish_keys",
    )
    rot_all = close(gather_pairs(rot_send, "tp", 8, (4, 2, 1)).reshape(GROUP, ROPE_DIM, TOK))
    (far_send,) = call(
        join_far,
        (exchange(weight_send, NEAR), close(dq)),
        [((GROUP, FAR_ROWS, TOK), BF, False)],
        "join_far",
    )
    query_grad, weight_grad, rot_grad = call(
        finish_rest,
        (exchange(far_send, BACK), rot_all),
        [((HEAD_DIM, TOK), BF, False), ((8, TOK), F32, False), ((ROPE_DIM, TOK), F32, False)],
        "finish_rest",
    )
    return query_grad.T, key_grad.T, value_grad.T, rot_grad.T, weight_grad


def solution(mesh):
    placed = (P("sp", "tp"), P("sp", None), P("sp", None), P(None, "tp"), P("sp", "tp"), P("sp", "tp"), P("sp", "tp"))
    step = jax.shard_map(
        per_device,
        mesh=mesh,
        in_specs=placed,
        out_specs=(P("sp", "tp"), P("sp", "tp"), P("sp", "tp"), P("sp", None), P("sp", "tp")),
        check_vma=False,
    )
    return step
```

```python
import math

import jax
import jax.numpy as jnp
from jax import lax
from jax.experimental import pallas as pl
from jax.experimental.pallas import tpu as pltpu
from jax.sharding import PartitionSpec as P


NOPE_DIM = 64
ROPE_DIM = 32
VALUE_DIM = 64
HEAD_DIM = NOPE_DIM + ROPE_DIM
SCALE = HEAD_DIM**-0.5
PAD = 8
FAR_ROWS = HEAD_DIM + 8
Q_ROWS = HEAD_DIM + PAD + VALUE_DIM
K_ROWS = HEAD_DIM + VALUE_DIM
BF = jnp.bfloat16
F32 = jnp.float32

OUT_ORDER = (8, 0, 12, 4, 10, 2, 14, 6)
BACK_ORDER = (0, 8, 4, 12, 2, 10, 6, 14)
OUT, BACK = (
    [[(z + low) * 4 + y for z in order] for low in range(2) for y in range(4)]
    for order in (OUT_ORDER, BACK_ORDER)
)
NEAR_ORDER = ((0, 0), (1, 0), (0, 2), (1, 2), (0, 1), (1, 1), (0, 3), (1, 3))
NEAR = [[(high + z) * 4 + y for z, y in NEAR_ORDER] for high in range(0, 16, 2)]
GROUP = 8
TOK = 128


def pairs(count, bit):
    return [[i, i + bit] for i in range(count) if not i & bit]


def three_parts(row):
    high = row.astype(BF)
    rest = row - high.astype(F32)
    middle = rest.astype(BF)
    low = (rest - middle.astype(F32)).astype(BF)
    return high.astype(F32), middle.astype(F32), low.astype(F32)


def prepare_keys(latents, rot_key, weight, k_out, latents_out):
    latents_out[...] = latents[...]
    joined = lax.dot_general(
        latents[...], weight[...], (((1,), (0,)), ((), ())), preferred_element_type=F32
    )
    joined_t = joined.T.astype(BF)
    k_out[:NOPE_DIM] = joined_t[:NOPE_DIM]
    k_out[NOPE_DIM:HEAD_DIM] = rot_key[...]
    k_out[HEAD_DIM:] = joined_t[NOPE_DIM:]


def prepare_queries(queries, logs, outputs, grads, q_out, block, sems):
    q_t = queries[...].astype(F32)
    g_t = grads[...].astype(F32)
    delta = jnp.sum(outputs[...].astype(F32) * g_t, axis=0, keepdims=True)
    rows = three_parts(logs[...] * (-1.0 / SCALE)) + three_parts(-delta)
    index = lax.broadcasted_iota(jnp.int32, (PAD, TOK), 0)
    pad = jnp.zeros((PAD, TOK), F32)
    for i, row in enumerate(rows):
        pad = jnp.where(index == i, row, pad)
    block[...] = jnp.concatenate([q_t, pad, g_t], axis=0).astype(BF)
    copies = [pltpu.make_async_copy(block, q_out.at[i], sems.at[i]) for i in range(GROUP)]
    for copy in copies:
        copy.start()
    for copy in copies:
        copy.wait()


def attend(q_all, k_all, dq_out, dkv_out, q_t, q_tok, g_tok, k_t, k_tok, v_tok, dq_acc, dk_acc, dv_acc, dscores, probs_b):
    total = GROUP * TOK
    lane = lax.broadcasted_iota(jnp.int32, (TOK, PAD), 1)
    key_pad = jnp.where(lane < 3, 1.0, 0.0).astype(F32)
    value_pad = jnp.where((lane >= 3) & (lane < 6), 1.0, 0.0).astype(F32)
    for i in range(GROUP):
        at = slice(i * TOK, (i + 1) * TOK)
        q_block = q_all[i]
        q_t[:, at] = q_block
        tok = q_block.astype(F32).T
        q_tok[at, :] = tok[:, :HEAD_DIM].astype(BF)
        g_tok[at, :] = tok[:, HEAD_DIM + PAD :].astype(BF)
        low, y = NEAR_ORDER[i]
        k_block = k_all[low * 4 + y]
        k_t[:, at] = k_block[:HEAD_DIM]
        ktok = k_block.astype(F32).T
        k_tok[at, :] = jnp.concatenate([ktok[:, :HEAD_DIM], key_pad], axis=1).astype(BF)
        v_tok[at, :] = jnp.concatenate([value_pad, ktok[:, HEAD_DIM:]], axis=1).astype(BF)
    step = 256
    for ki in range(total // step):
        ks = slice(ki * step, (ki + 1) * step)
        for qi in range(total // step):
            qs = slice(qi * step, (qi + 1) * step)
            scores = jnp.dot(k_tok[ks, :], q_t[: HEAD_DIM + PAD, qs], preferred_element_type=F32)
            probs = jnp.exp2(scores * (SCALE * math.log2(math.e)))
            dprob = jnp.dot(v_tok[ks, :], q_t[HEAD_DIM:, qs], preferred_element_type=F32)
            dscores[ks, qs] = (probs * dprob).astype(BF)
            probs_b[ks, qs] = probs.astype(BF)
        dk_acc[ks, :] = jnp.dot(dscores[ks, :], q_tok[...], preferred_element_type=F32)
        dv_acc[ks, :] = jnp.dot(probs_b[ks, :], g_tok[...], preferred_element_type=F32)
    for qi in range(total // step):
        qs = slice(qi * step, (qi + 1) * step)
        dq_acc[:, qs] = jnp.dot(k_t[...], dscores[:, qs], preferred_element_type=F32)
    for i in range(GROUP):
        at = slice(i * TOK, (i + 1) * TOK)
        dq_out[BACK_ORDER.index(OUT_ORDER[i])] = (dq_acc[:, at] * SCALE).astype(BF)
        dkv_out[i] = jnp.concatenate(
            [(dk_acc[at, :] * SCALE).T, dv_acc[at, :].T], axis=0
        ).astype(BF)


def finish_keys(dkv, latents, key_grad, value_grad, rot_out, weight_out):
    total = dkv[0].astype(F32)
    for i in range(1, GROUP):
        total = total + dkv[i].astype(F32)
    rot_out[...] = total[NOPE_DIM:HEAD_DIM]
    key_grad[...] = total[:NOPE_DIM].astype(BF)
    value_grad[...] = total[HEAD_DIM:].astype(BF)
    stacked = jnp.concatenate([total[:NOPE_DIM], total[HEAD_DIM:]], axis=0).T.astype(BF)
    weight = lax.dot_general(
        latents[...], stacked, (((0,), (0,)), ((), ())), preferred_element_type=F32
    )
    by_owner = weight.reshape(GROUP, GROUP, 8, TOK)
    for i in range(GROUP):
        low, y = NEAR_ORDER[i]
        rows = [by_owner[z // 2, low * 4 + y] for z in BACK_ORDER]
        weight_out[i] = jnp.concatenate(rows, axis=0).astype(BF)


def join_far(weight, dq, far_out):
    total = weight[0].astype(F32)
    for i in range(1, GROUP):
        total = total + weight[i].astype(F32)
    for i in range(GROUP):
        far_out[i, :HEAD_DIM] = dq[i]
        far_out[i, HEAD_DIM:] = total[i * 8 : (i + 1) * 8].astype(BF)


def finish_rest(far, rot, query_grad, weight_grad, rot_grad):
    total = far[0].astype(F32)
    around = rot[0]
    for i in range(1, GROUP):
        total = total + far[i].astype(F32)
        around = around + rot[i]
    query_grad[...] = total[:HEAD_DIM].astype(BF)
    weight_grad[...] = total[HEAD_DIM:]
    rot_grad[...] = around


def call(body, args, outs, name, scratch=(), **more):
    shapes = [
        pltpu.VMEM(shape, kind) if near else jax.ShapeDtypeStruct(shape, kind)
        for shape, kind, near in outs
    ]
    return pl.pallas_call(body, out_shape=shapes, scratch_shapes=list(scratch), name=name, **more)(
        *args
    )


def close(x):
    return pltpu.with_memory_space_constraint(x, pltpu.VMEM)


def exchange(x, groups):
    return close(lax.all_to_all(x, "sp", 0, 0, axis_index_groups=groups, tiled=True))


def gather_pairs(x, axis, count, bits):
    for bit in bits:
        x = lax.all_gather(x, axis, axis_index_groups=pairs(count, bit))
    return x


def per_device(queries, latents, rot_key, kv_weight, log_sums, outputs, out_grad):
    total = GROUP * TOK
    (q_send,) = call(
        prepare_queries,
        (queries.T, log_sums.T, outputs.T, out_grad.T),
        [((GROUP, Q_ROWS, TOK), BF, False)],
        "prepare_queries",
        [pltpu.VMEM((Q_ROWS, TOK), BF), pltpu.SemaphoreType.DMA((GROUP,))],
        out_specs=[pl.BlockSpec(memory_space=pl.ANY)],
    )
    k_send, latents_kept = call(
        prepare_keys,
        (latents, rot_key.T, kv_weight),
        [((K_ROWS, TOK), BF, True), (latents.shape, BF, True)],
        "prepare_keys",
    )
    q_all = exchange(q_send, OUT)
    k_all = close(gather_pairs(k_send, "sp", 64, (1, 2, 4)).reshape(GROUP, K_ROWS, TOK))
    dq, dkv = call(
        attend,
        (q_all, k_all),
        [((GROUP, HEAD_DIM, TOK), BF, True), ((GROUP, K_ROWS, TOK), BF, True)],
        "attend",
        [
            pltpu.VMEM((Q_ROWS, total), BF),
            pltpu.VMEM((total, HEAD_DIM), BF),
            pltpu.VMEM((total, VALUE_DIM), BF),
            pltpu.VMEM((HEAD_DIM, total), BF),
            pltpu.VMEM((total, HEAD_DIM + PAD), BF),
            pltpu.VMEM((total, PAD + VALUE_DIM), BF),
            pltpu.VMEM((HEAD_DIM, total), F32),
            pltpu.VMEM((total, HEAD_DIM), F32),
            pltpu.VMEM((total, VALUE_DIM), F32),
            pltpu.VMEM((total, total), BF),
            pltpu.VMEM((total, total), BF),
        ],
    )
    key_grad, value_grad, rot_send, weight_send = call(
        finish_keys,
        (exchange(dkv, NEAR), close(latents_kept)),
        [
            ((NOPE_DIM, TOK), BF, False),
            ((VALUE_DIM, TOK), BF, False),
            ((ROPE_DIM, TOK), F32, True),
            ((GROUP, GROUP * 8, TOK), BF, True),
        ],
        "finish_keys",
    )
    rot_all = close(gather_pairs(rot_send, "tp", 8, (4, 2, 1)).reshape(GROUP, ROPE_DIM, TOK))
    (far_send,) = call(
        join_far,
        (exchange(weight_send, NEAR), close(dq)),
        [((GROUP, FAR_ROWS, TOK), BF, False)],
        "join_far",
    )
    query_grad, weight_grad, rot_grad = call(
        finish_rest,
        (exchange(far_send, BACK), rot_all),
        [((HEAD_DIM, TOK), BF, False), ((8, TOK), F32, False), ((ROPE_DIM, TOK), F32, False)],
        "finish_rest",
    )
    return query_grad.T, key_grad.T, value_grad.T, rot_grad.T, weight_grad


def solution(mesh):
    placed = (P("sp", "tp"), P("sp", None), P("sp", None), P(None, "tp"), P("sp", "tp"), P("sp", "tp"), P("sp", "tp"))
    step = jax.shard_map(
        per_device,
        mesh=mesh,
        in_specs=placed,
        out_specs=(P("sp", "tp"), P("sp", "tp"), P("sp", "tp"), P("sp", None), P("sp", "tp")),
        check_vma=False,
    )
    return step
```
